512 devices in a mesh: kv: 16 (over y, x), tp: 32 (over z, core).
Axes of the slice: x: 4, y: 4, z: 16, core: 2. Of those that a mesh axis runs over, the one named last changes fastest.
Arguments:
- hidden_in: bfloat16 [64, 4096], P('kv', 'tp'), may hold values from -12 to 12
- mixer_gain: float32 [4096], P('tp'), may hold values from 0.1 to 1.9
- query_weight: bfloat16 [4096, 4096], P('tp', 'kv'), may hold values from -0.09375 to 0.09375
- key_weight: bfloat16 [4096, 4096], P('tp', 'kv'), may hold values from -0.09375 to 0.09375
- value_weight: bfloat16 [4096, 8192], P('tp', 'kv'), may hold values from -0.09375 to 0.09375
- gate_weight: bfloat16 [4096, 8192], P('tp', 'kv'), may hold values from -0.09375 to 0.09375
- decay_rate: float32 [16], P('kv'), may hold values from 0.0005 to 0.15
- prior_state: float32 [64, 16, 256, 512], P('tp', 'kv'), may hold values from -2.5 to 2.5
- key_block: bfloat16 [64, 16, 128, 256], P('tp', 'kv'), may hold values from -1 to 1
- value_block: bfloat16 [64, 16, 128, 512], P('tp', 'kv'), may hold values from -6 to 6
- lengths: int32 [64], P('tp'), may hold values from 1 to 16384, 262144 in all
- group_gain: float32 [8192], P('kv'), may hold values from 0.1 to 1.9
- output_weight: bfloat16 [8192, 4096], P('kv', 'tp'), may hold values from -0.0625 to 0.0625
- channel_gain: float32 [4096], P('tp'), may hold values from 0.1 to 1.9
- hidden_gate: bfloat16 [4096, 11264], P('tp', 'kv'), may hold values from -0.09375 to 0.09375
- hidden_up: bfloat16 [4096, 11264], P('tp', 'kv'), may hold values from -0.09375 to 0.09375
- hidden_down: bfloat16 [11264, 4096], P('kv', 'tp'), may hold values from -0.0546875 to 0.0546875
Outputs:
- layer_out: bfloat16 [64, 4096], P('kv', 'tp')
The draws below stay inside these ranges and needn't reach their ends.
Inputs may be any that keep to these rules, and one draw needn't show every extreme that they name: Sequence s has lengths[s] earlier positions; slots 0 to (lengths[s] mod 128) - 1 of key_block and value_block hold the turned, scaled keys and the values of its positions from 128 * floor(lengths[s] / 128) on, prior_state holds the state of the positions before them, and the other slots take no part.
All inputs are finite; a program needn't handle non-finite values. No bound on the sum of `lengths` on one device may be relied on, other than what follows from the above.
Results may differ from the reference program's by a relative error of at most 0.029.
Values may be sent and summed in bfloat16 or wider, within the bound.
No kernel may reach another device: no remote copies, remote signals or barrier semaphores. Data moves between devices by JAX's collectives and lax.ppermute only.
A program may use at most 64 MiB of HBM per device.

```python
import math
import jax
import jax.numpy as jnp
import numpy as np
from jax import lax

D = 4096
HEADS = 16
DK = 256
DV = 512
FF = 11264
BLK = 128
MEAN_LEN = 4096
MOST_LEN = 16384
SEQS = 64


def draw_hidden_in(key, part):
    columns = jnp.arange(D, dtype=jnp.float32) / D
    column_scale = 0.4 * jnp.exp(jnp.log(5.0) * columns)
    base_key = jax.random.fold_in(key, 11)
    base = jnp.clip(jax.random.normal(base_key, (SEQS, D), jnp.float32), -6.0, 6.0)
    return (base * column_scale[None, :]).astype(jnp.bfloat16)


def draw_decay_rate(key, part):
    lowest_rate = 0.003
    highest_rate = 0.15
    uniform_unit = jax.random.uniform(jax.random.fold_in(key, 21), (HEADS,), jnp.float32)
    return jnp.exp(jnp.log(lowest_rate) + uniform_unit * (jnp.log(highest_rate) - jnp.log(lowest_rate)))


def steps_of(own_key, extent, pieces, smallest, high):
    gain = 1.0
    for dim, shards_of in pieces:
        draws = jax.random.uniform(jax.random.fold_in(jax.random.fold_in(own_key, 6), dim), (shards_of,), jnp.float32, smallest / len(pieces), high / len(pieces))
        gain = gain * jnp.repeat(jnp.exp(draws), extent[dim] // shards_of).reshape((-1,) + (1,) * (len(extent) - 1 - dim))
    return gain


def length_profile(number_of, total, limit, lean):
    weights = [(1 << 20) // math.isqrt(standing ** lean) + 1 for standing in range(2, number_of + 1)]
    spare, counts = total - limit - (number_of - 1), [1] * (number_of - 1)
    while spare > 0:
        free = [i for i in range(number_of - 1) if counts[i] < limit]
        whole, budget = sum([weights[i] for i in free]), spare
        for i in free:
            extra = min(limit - counts[i], max(1, budget * weights[i] // whole), spare)
            counts[i] = counts[i] + extra
            spare = spare - extra
    return np.array([limit] + counts)


def uneven_parts(key, number_of, total, limit, skew):
    if number_of == 2:
        one = jax.random.randint(key, (), max(1, total - limit), min(limit, total - 1) + 1)
        return jnp.stack([one, total - one])
    sizes = jnp.asarray(length_profile(number_of, total, limit, skew), jnp.int32)
    couples = (number_of - 1) // 2
    giver, taker = sizes[1:1 + 2 * couples:2], sizes[2:2 + 2 * couples:2]
    room = jnp.minimum(giver - 1, limit - taker)
    shifted = jax.random.randint(jax.random.fold_in(key, 1), (couples,), 0, 1 << 20) % (room + 1)
    sizes = sizes.at[1:1 + 2 * couples:2].set(giver - shifted).at[2:2 + 2 * couples:2].set(taker + shifted)
    return sizes[jax.random.permutation(jax.random.fold_in(key, 2), number_of)]


def bell_draw(stream_key, extent, deviation, limit, split=(), kind=jnp.bfloat16):
    drawn = jax.random.normal(stream_key, extent, jnp.float32) * deviation
    if len(split) > 0:
        drawn = steps_of(stream_key, extent, split, -0.22, 0.18) * drawn
    return jnp.clip(drawn, min=-limit, max=limit).astype(kind)


def setup_inputs(seed: int = 0) -> dict:
    keys = jax.random.split(jax.random.key(seed), 18)
    return {
        "hidden_in": draw_hidden_in(jax.random.fold_in(keys[17], 71), 0),
        "mixer_gain": jnp.clip(1.0 + 0.18 * jax.random.normal(keys[1], (D,), jnp.float32), 0.1, 1.9),
        "query_weight": bell_draw(keys[2], (D, HEADS * DK), D ** -0.5, 0.09375, ((0, 32), (1, 16))),
        "key_weight": bell_draw(keys[3], (D, HEADS * DK), D ** -0.5, 0.09375, ((0, 32), (1, 16))),
        "value_weight": bell_draw(keys[4], (D, HEADS * DV), D ** -0.5, 0.09375, ((0, 32), (1, 16))),
        "gate_weight": bell_draw(keys[5], (D, HEADS * DV), D ** -0.5, 0.09375, ((0, 32), (1, 16))),
        "decay_rate": draw_decay_rate(jax.random.fold_in(keys[17], 71), 0),
        "prior_state": bell_draw(keys[7], (SEQS, HEADS, DK, DV), 0.3, 2.5, ((0, 32), (1, 16)), jnp.float32),
        "key_block": bell_draw(keys[8], (SEQS, HEADS, BLK, DK), 0.0625, 1.0, ((0, 32), (1, 16))),
        "value_block": bell_draw(keys[9], (SEQS, HEADS, BLK, DV), 1.0, 6.0, ((0, 32), (1, 16))),
        "lengths": uneven_parts(keys[10], SEQS, SEQS * MEAN_LEN, MOST_LEN, 2).astype(jnp.int32),
        "group_gain": jnp.clip(1.0 + 0.18 * jax.random.normal(keys[11], (HEADS * DV,), jnp.float32), 0.1, 1.9),
        "output_weight": bell_draw(keys[12], (HEADS * DV, D), (HEADS * DV) ** -0.5, 0.0625, ((0, 16), (1, 32))),
        "channel_gain": jnp.clip(1.0 + 0.18 * jax.random.normal(keys[13], (D,), jnp.float32), 0.1, 1.9),
        "hidden_gate": bell_draw(keys[14], (D, FF), D ** -0.5, 0.09375, ((0, 32), (1, 16))),
        "hidden_up": bell_draw(keys[15], (D, FF), D ** -0.5, 0.09375, ((0, 32), (1, 16))),
        "hidden_down": bell_draw(keys[16], (FF, D), FF ** -0.5, 0.0546875, ((0, 16), (1, 32))),
    }


epsilon = 1e-06

def rotate(vectors, position):
    half_dim = vectors.shape[-1] // 2
    inverse = 10000.0 ** (-jnp.arange(half_dim, dtype=jnp.float32) / half_dim)
    angles = position.astype(jnp.float32)[:, None, None] * inverse
    cosine_part = jnp.cos(angles)
    sine_part = jnp.sin(angles)
    front_half = vectors[..., :half_dim]
    back_half = vectors[..., half_dim:]
    return jnp.concatenate([front_half * cosine_part - back_half * sine_part, front_half * sine_part + back_half * cosine_part], axis=-1)

def retain(queries, keys_new, values_new, gates, decay_rate, prior_state, key_block, value_block, lengths, group_gain):
    batch_rows = queries.shape[0]
    heads_here = decay_rate.shape[0]
    key_width = prior_state.shape[2]
    value_width = prior_state.shape[3]
    block_len = key_block.shape[2]
    rotated = rotate(queries.astype(jnp.float32).reshape(batch_rows, heads_here, key_width), lengths).astype(jnp.bfloat16)
    fresh_keys = rotate(keys_new.astype(jnp.float32).reshape(batch_rows, heads_here, key_width), lengths) * key_width ** (-0.5)
    fresh_values = values_new.astype(jnp.float32).reshape(batch_rows, heads_here, value_width)
    filled = (lengths % block_len).astype(jnp.int32)
    slots = jnp.arange(block_len, dtype=jnp.int32)
    distance = (filled[:, None] - slots[None, :]).astype(jnp.float32)
    live_slots = (slots[None, :] < filled[:, None])[:, None, :]
    weighting = jnp.where(live_slots, jnp.exp(-decay_rate[None, :, None] * distance[:, None, :]), jnp.float32(0.0))
    rotated_wide = rotated.astype(jnp.float32)
    scores = jnp.einsum('shk,shjk->shj', rotated_wide, key_block.astype(jnp.float32))
    block_weights = (scores * weighting).astype(jnp.bfloat16)
    block_term = jnp.einsum('shj,shjv->shv', block_weights.astype(jnp.float32), value_block.astype(jnp.float32))
    own_term = lax.optimization_barrier(jnp.sum(rotated_wide * fresh_keys, axis=-1, keepdims=True)) * fresh_values
    carried = jnp.exp(-decay_rate[None, :, None] * (filled[:, None, None] + 1).astype(jnp.float32))
    state_term = carried * jnp.einsum('shk,shkv->shv', rotated_wide, prior_state, precision=lax.Precision.HIGHEST)
    retained = own_term + block_term + state_term
    centre = lax.optimization_barrier(jnp.mean(retained, axis=-1, keepdims=True))
    spread = lax.optimization_barrier(jnp.mean(jnp.square(retained - centre), axis=-1, keepdims=True))
    normed = (retained - centre) * lax.rsqrt(spread + epsilon)
    gated = jax.nn.silu(gates.astype(jnp.float32)).reshape(batch_rows, heads_here, value_width) * normed * group_gain.reshape(heads_here, value_width)
    return gated.astype(jnp.bfloat16).reshape(batch_rows, heads_here * value_width)

def reference(hidden_in, mixer_gain, query_weight, key_weight, value_weight, gate_weight, decay_rate, prior_state, key_block, value_block, lengths, group_gain, output_weight, channel_gain, hidden_gate, hidden_up, hidden_down):
    stream = hidden_in.astype(jnp.float32)
    first_scale = lax.rsqrt(lax.optimization_barrier(jnp.mean(stream * stream, axis=1, keepdims=True)) + epsilon)
    scaled_in = (stream * mixer_gain).astype(jnp.bfloat16)
    queries = (first_scale * jnp.dot(scaled_in, query_weight, preferred_element_type=jnp.float32)).astype(jnp.bfloat16)
    keys_new = (first_scale * jnp.dot(scaled_in, key_weight, preferred_element_type=jnp.float32)).astype(jnp.bfloat16)
    values_new = (first_scale * jnp.dot(scaled_in, value_weight, preferred_element_type=jnp.float32)).astype(jnp.bfloat16)
    gates = (first_scale * jnp.dot(scaled_in, gate_weight, preferred_element_type=jnp.float32)).astype(jnp.bfloat16)
    mixed = retain(queries, keys_new, values_new, gates, decay_rate, prior_state, key_block, value_block, lengths, group_gain)
    middle = stream + jnp.dot(mixed, output_weight, preferred_element_type=jnp.float32)
    second_scale = lax.rsqrt(lax.optimization_barrier(jnp.mean(middle * middle, axis=1, keepdims=True)) + epsilon)
    scaled_mid = (middle * channel_gain).astype(jnp.bfloat16)
    gate_part = second_scale * jnp.dot(scaled_mid, hidden_gate, preferred_element_type=jnp.float32)
    up_part = second_scale * jnp.dot(scaled_mid, hidden_up, preferred_element_type=jnp.float32)
    activated = (jax.nn.silu(gate_part) * up_part).astype(jnp.bfloat16)
    return (middle + jnp.dot(activated, hidden_down, preferred_element_type=jnp.float32)).astype(jnp.bfloat16)
```

```python
import jax
import jax.numpy as jnp
from jax import lax
from jax.sharding import PartitionSpec as P

D = 4096
LANES = 128


epsilon = 1e-06


def from_everyone(value, axis):
    copies = jnp.broadcast_to(value, (lax.axis_size(axis), *value.shape))
    return lax.all_to_all(copies, axis, split_axis=0, concat_axis=0, tiled=True)


def in_order(parts, dim):
    shape = list(parts.shape[1:])
    shape[dim] *= parts.shape[0]
    return jnp.moveaxis(parts, 0, dim).reshape(shape)


def gathered_copies(value, axis, dim):
    parts = from_everyone(value, axis)
    return in_order(parts, dim)


def split_up(value, dim, count):
    shape = value.shape
    parts = value.reshape(*shape[:dim], count, shape[dim] // count, *shape[dim + 1 :])
    return jnp.moveaxis(parts, dim, 0)


def summed_on_arrival(value, axis, dim):
    count = lax.axis_size(axis)
    parts = lax.all_to_all(split_up(value, dim, count), axis, 0, 0, tiled=True)
    return jnp.sum(parts.astype(jnp.float32), axis=0)


def side_by_side(arrays, axis, dim, along):
    ends, at = ([], 0)
    for a in arrays[:-1]:
        at += a.shape[along]
        ends.append(at)
    both = jnp.concatenate(arrays, axis=along)
    return tuple(jnp.split(summed_on_arrival(both, axis, dim), ends, axis=along))


def as_column(value, width):
    return jnp.pad(value, ((0, 0), (0, width - 1))).astype(jnp.bfloat16)


def rotate(vectors, position):
    half_dim = vectors.shape[-1] // 2
    inverse = 10000.0 ** (-jnp.arange(half_dim, dtype=jnp.float32) / half_dim)
    angles = position.astype(jnp.float32)[:, None, None] * inverse
    cosine_part = jnp.cos(angles)
    sine_part = jnp.sin(angles)
    front_half = vectors[..., :half_dim]
    back_half = vectors[..., half_dim:]
    return jnp.concatenate(
        [
            front_half * cosine_part - back_half * sine_part,
            front_half * sine_part + back_half * cosine_part,
        ],
        axis=-1,
    )


def retain(
    queries,
    keys_new,
    values_new,
    gates,
    decay_rate,
    prior_state,
    key_block,
    value_block,
    lengths,
    group_gain,
):
    batch_rows = queries.shape[0]
    heads_here = decay_rate.shape[0]
    key_width = prior_state.shape[2]
    value_width = prior_state.shape[3]
    block_len = key_block.shape[2]
    rotated = rotate(
        queries.astype(jnp.float32).reshape(batch_rows, heads_here, key_width), lengths
    ).astype(jnp.bfloat16)
    fresh_keys = rotate(
        keys_new.astype(jnp.float32).reshape(batch_rows, heads_here, key_width), lengths
    ) * key_width ** (-0.5)
    fresh_values = values_new.astype(jnp.float32).reshape(batch_rows, heads_here, value_width)
    filled = lengths % block_len
    slots = jnp.arange(block_len, dtype=jnp.int32)
    distance = (filled[:, None] - slots[None, :]).astype(jnp.float32)
    live_slots = (slots[None, :] < filled[:, None])[:, None, :]
    weighting = jnp.where(
        live_slots, jnp.exp(-decay_rate[None, :, None] * distance[:, None, :]), jnp.float32(0.0)
    )
    scores = jnp.einsum("shk,shjk->shj", rotated, key_block, preferred_element_type=jnp.float32)
    block_weights = (scores * weighting).astype(jnp.bfloat16)
    block_term = jnp.einsum(
        "shj,shjv->shv", block_weights, value_block, preferred_element_type=jnp.float32
    )
    rotated_wide = rotated.astype(jnp.float32)
    own_term = jnp.sum(rotated_wide * fresh_keys, axis=-1, keepdims=True) * fresh_values
    carried = jnp.exp(-decay_rate[None, :, None] * (filled[:, None, None] + 1).astype(jnp.float32))
    state_term = carried * jnp.einsum(
        "shk,shkv->shv", rotated_wide, prior_state, precision=lax.Precision.HIGHEST
    )
    retained = own_term + block_term + state_term
    centre = jnp.mean(retained, axis=-1, keepdims=True)
    spread = jnp.mean(jnp.square(retained - centre), axis=-1, keepdims=True)
    normed = (retained - centre) * lax.rsqrt(spread + epsilon)
    gated = (
        jax.nn.silu(gates.astype(jnp.float32)).reshape(batch_rows, heads_here, value_width)
        * normed
        * group_gain.reshape(heads_here, value_width)
    )
    return gated.astype(jnp.bfloat16).reshape(batch_rows, heads_here * value_width)


def local(
    hidden_in,
    mixer_gain,
    query_weight,
    key_weight,
    value_weight,
    gate_weight,
    decay_rate,
    prior_state,
    key_block,
    value_block,
    lengths,
    group_gain,
    output_weight,
    channel_gain,
    hidden_gate,
    hidden_up,
    hidden_down,
):
    own_rows = hidden_in.shape[0]
    units = hidden_gate.shape[1]
    pad = -units % LANES
    stream = gathered_copies(hidden_in, "kv", 0).astype(jnp.float32)
    scaled_in = (stream * mixer_gain).astype(jnp.bfloat16)
    squares = as_column(jnp.sum(stream * stream, axis=1, keepdims=True), LANES)
    terms = [
        jnp.dot(scaled_in, matrix, preferred_element_type=jnp.float32).astype(jnp.bfloat16)
        for matrix in (query_weight, key_weight, value_weight, gate_weight)
    ]
    queries, keys_new, values_new, gates, row_squares = side_by_side(
        (*terms, squares), "tp", 0, 1
    )
    first_scale = lax.rsqrt(row_squares[:, :1] / D + epsilon)
    queries = (first_scale * queries).astype(jnp.bfloat16)
    keys_new = (first_scale * keys_new).astype(jnp.bfloat16)
    values_new = (first_scale * values_new).astype(jnp.bfloat16)
    gates = (first_scale * gates).astype(jnp.bfloat16)
    mixed = retain(
        queries,
        keys_new,
        values_new,
        gates,
        decay_rate,
        prior_state,
        key_block,
        value_block,
        lengths,
        group_gain,
    )
    head_terms = jnp.dot(
        gathered_copies(mixed, "tp", 0), output_weight, preferred_element_type=jnp.float32
    )
    head_parts = from_everyone(head_terms.astype(jnp.bfloat16), "kv")
    middle = stream + jnp.sum(head_parts.astype(jnp.float32), axis=0)
    scaled_mid = (middle * channel_gain).astype(jnp.bfloat16)
    middle_squares = as_column(jnp.sum(middle * middle, axis=1, keepdims=True), pad)
    gate_terms, up_terms = (
        jnp.dot(scaled_mid, matrix, preferred_element_type=jnp.float32).astype(jnp.bfloat16)
        for matrix in (hidden_gate, hidden_up)
    )
    channel_summed = summed_on_arrival(
        jnp.concatenate([gate_terms, middle_squares, up_terms], axis=1), "tp", 0
    )
    second_scale = lax.rsqrt(channel_summed[:, units : units + 1] / D + epsilon)
    gate_part = second_scale * channel_summed[:, :units]
    up_part = second_scale * channel_summed[:, units + pad :]
    activated = (jax.nn.silu(gate_part) * up_part).astype(jnp.bfloat16)
    unit_terms = jnp.dot(
        gathered_copies(activated, "tp", 0), hidden_down, preferred_element_type=jnp.float32
    )
    channel_out = summed_on_arrival(unit_terms.astype(jnp.bfloat16), "kv", 0)
    own_middle = lax.dynamic_slice_in_dim(middle, lax.axis_index("kv") * own_rows, own_rows, 0)
    return (own_middle + channel_out).astype(jnp.bfloat16)


def solution(mesh):
    in_specs = (
        P("kv", "tp"),
        P("tp"),
        P("tp", "kv"),
        P("tp", "kv"),
        P("tp", "kv"),
        P("tp", "kv"),
        P("kv"),
        P("tp", "kv", None, None),
        P("tp", "kv", None, None),
        P("tp", "kv", None, None),
        P("tp"),
        P("kv"),
        P("kv", "tp"),
        P("tp"),
        P("tp", "kv"),
        P("tp", "kv"),
        P("kv", "tp"),
    )
    out_specs = P("kv", "tp")
    return jax.shard_map(local, mesh=mesh, in_specs=in_specs, out_specs=out_specs, check_vma=False)
```

```python
import jax
import jax.numpy as jnp
from jax import lax
from jax.sharding import Mesh
from jax.sharding import PartitionSpec as P

D = 4096
LANES = 128


epsilon = 1e-06


def exchange(parts, axes):
    return lax.all_to_all(parts, axes, split_axis=0, concat_axis=0, tiled=True)


def copies(value, count):
    return jnp.broadcast_to(value, (count, *value.shape))


def from_partner(value):
    return lax.ppermute(value, "core", [(0, 1), (1, 0)])


def wide_dot(left, right):
    return jnp.dot(left, right, preferred_element_type=jnp.float32)


def as_column(value, width):
    return jnp.pad(value, ((0, 0), (0, width - 1))).astype(jnp.bfloat16)


def thirds(value):
    high = lax.reduce_precision(value, 8, 7)
    rest = value - high
    middle = lax.reduce_precision(rest, 8, 7)
    return [part.astype(jnp.bfloat16) for part in (high, middle, rest - middle)]


def rotate(vectors, position):
    half_dim = vectors.shape[-1] // 2
    inverse = 10000.0 ** (-jnp.arange(half_dim, dtype=jnp.float32) / half_dim)
    angles = position.astype(jnp.float32)[:, None, None] * inverse
    cosine_part = jnp.cos(angles)
    sine_part = jnp.sin(angles)
    front_half = vectors[..., :half_dim]
    back_half = vectors[..., half_dim:]
    return jnp.concatenate(
        [
            front_half * cosine_part - back_half * sine_part,
            front_half * sine_part + back_half * cosine_part,
        ],
        axis=-1,
    )


def retain(
    queries,
    keys_new,
    values_new,
    gates,
    decay_rate,
    prior_state,
    key_block,
    value_block,
    lengths,
    group_gain,
):
    batch_rows = queries.shape[0]
    heads_here = decay_rate.shape[0]
    key_width = prior_state.shape[2]
    value_width = prior_state.shape[3]
    block_len = key_block.shape[2]
    rotated = rotate(
        queries.astype(jnp.float32).reshape(batch_rows, heads_here, key_width), lengths
    ).astype(jnp.bfloat16)
    fresh_keys = rotate(
        keys_new.astype(jnp.float32).reshape(batch_rows, heads_here, key_width), lengths
    ) * key_width ** (-0.5)
    fresh_values = values_new.astype(jnp.float32).reshape(batch_rows, heads_here, value_width)
    filled = lengths % block_len
    slots = jnp.arange(block_len, dtype=jnp.int32)
    distance = (filled[:, None] - slots[None, :]).astype(jnp.float32)
    live_slots = (slots[None, :] < filled[:, None])[:, None, :]
    weighting = jnp.where(
        live_slots, jnp.exp(-decay_rate[None, :, None] * distance[:, None, :]), jnp.float32(0.0)
    )
    scores = jnp.einsum("shk,shjk->shj", rotated, key_block, preferred_element_type=jnp.float32)
    block_weights = (scores * weighting).astype(jnp.bfloat16)
    block_term = jnp.einsum(
        "shj,shjv->shv", block_weights, value_block, preferred_element_type=jnp.float32
    )
    rotated_wide = rotated.astype(jnp.float32)
    own_term = jnp.sum(rotated_wide * fresh_keys, axis=-1, keepdims=True) * fresh_values
    carried = jnp.exp(-decay_rate[None, :, None] * (filled[:, None, None] + 1).astype(jnp.float32))
    state_term = carried * jnp.einsum(
        "shk,shkv->shv", rotated_wide, prior_state, precision=lax.Precision.HIGHEST
    )
    retained = own_term + block_term + state_term
    centre = jnp.mean(retained, axis=-1, keepdims=True)
    spread = jnp.mean(jnp.square(retained - centre), axis=-1, keepdims=True)
    normed = (retained - centre) * lax.rsqrt(spread + epsilon)
    gated = (
        jax.nn.silu(gates.astype(jnp.float32)).reshape(batch_rows, heads_here, value_width)
        * normed
        * group_gain.reshape(heads_here, value_width)
    )
    return gated.astype(jnp.bfloat16).reshape(batch_rows, heads_here * value_width)


def local(
    hidden_in,
    mixer_gain,
    query_weight,
    key_weight,
    value_weight,
    gate_weight,
    decay_rate,
    prior_state,
    key_block,
    value_block,
    lengths,
    group_gain,
    output_weight,
    channel_gain,
    hidden_gate,
    hidden_up,
    hidden_down,
):
    kv, z = lax.axis_size("kv"), lax.axis_size("z")
    core = lax.axis_index("core")
    own_rows, features = hidden_in.shape
    half = own_rows // 2
    rows = kv * half
    key_width, value_width = query_weight.shape[1], value_weight.shape[1]
    head_width, units = output_weight.shape[0], hidden_gate.shape[1]
    pad = -units % LANES

    def own_and_partner(pair):
        swapped = core == 1
        return (
            jnp.where(swapped, pair[1], pair[0]),
            jnp.where(swapped, pair[0], pair[1]),
        )

    with jax.named_scope("rows"):
        scaled = (hidden_in.astype(jnp.float32) * mixer_gain).astype(jnp.bfloat16)
        by_core = jnp.concatenate(
            [hidden_in.reshape(2, half, features), scaled.reshape(2, half, features)], axis=1
        )
        sent = jnp.broadcast_to(by_core[:, None], (2, kv, 2 * half, features))
        arrived = exchange(sent.reshape(2 * kv, 2 * half, features), ("core", "kv"))
        arrived = arrived.reshape(2, kv, 2 * half, features)
    with jax.named_scope("swap_first"):
        first_own = jnp.concatenate([query_weight, key_weight, value_weight, gate_weight], axis=1)
        first_partner = from_partner(first_own)
    with jax.named_scope("swap_second"):
        second_partner = from_partner(
            jnp.concatenate(
                [
                    output_weight,
                    hidden_gate.T,
                    hidden_up.T,
                    hidden_down,
                    jnp.pad(jnp.stack(thirds(channel_gain)), ((0, 13), (0, 0))),
                ],
                axis=0,
            )
        )
        at = head_width + 3 * units
        partner_output = second_partner[:head_width]
        partner_gate = second_partner[head_width : head_width + units]
        partner_up = second_partner[head_width + units : head_width + 2 * units]
        partner_down = second_partner[head_width + 2 * units : at]
        partner_gain = jnp.sum(second_partner[at : at + 3].astype(jnp.float32), axis=0)

    with jax.named_scope("project"):
        stream = own_and_partner(
            arrived[:, :, :half].reshape(2, rows, features).astype(jnp.float32)
        )
        scaled_in = own_and_partner(arrived[:, :, half:].reshape(2, rows, features))
        squares = sum(jnp.sum(part * part, axis=1, keepdims=True) for part in stream)
        terms = wide_dot(scaled_in[0], first_own) + wide_dot(scaled_in[1], first_partner)
        terms = jnp.concatenate([terms.astype(jnp.bfloat16), as_column(squares, LANES)], axis=1)
        arrived = exchange(terms.reshape(z, half, -1), "z")
        summed = jnp.sum(arrived.astype(jnp.float32), axis=0)
    with jax.named_scope("retain"):
        ends = [key_width, 2 * key_width, 2 * key_width + value_width]
        ends.append(ends[-1] + value_width)
        *projected, row_squares = jnp.split(summed, ends, axis=1)
        first_scale = lax.rsqrt(row_squares[:, :1] / D + epsilon)
        projected = [(first_scale * part).astype(jnp.bfloat16) for part in projected]
        mixed = retain(
            *projected,
            decay_rate,
            prior_state,
            key_block,
            value_block,
            lengths,
            group_gain,
        )
    with jax.named_scope("mix"):
        all_mixed = exchange(copies(mixed, z), "z").reshape(rows, head_width)
        head_terms = jnp.concatenate(
            [wide_dot(all_mixed, output_weight), wide_dot(all_mixed, partner_output)], axis=1
        ).astype(jnp.bfloat16)
        head_parts = exchange(copies(head_terms, kv), "kv")
        mixer_out = jnp.sum(head_parts.astype(jnp.float32), axis=0)
    with jax.named_scope("channel"):
        middle = [
            part + out for part, out in zip(stream, jnp.split(mixer_out, 2, axis=1))
        ]
        scaled_own = (middle[0] * channel_gain).astype(jnp.bfloat16)
        scaled_partner = (middle[1] * partner_gain).astype(jnp.bfloat16)
        middle_squares = sum(jnp.sum(part * part, axis=1, keepdims=True) for part in middle)
        gate_terms = wide_dot(scaled_own, hidden_gate) + wide_dot(scaled_partner, partner_gate.T)
        up_terms = wide_dot(scaled_own, hidden_up) + wide_dot(scaled_partner, partner_up.T)
        channel_terms = jnp.concatenate(
            [
                gate_terms.astype(jnp.bfloat16),
                as_column(middle_squares, pad),
                up_terms.astype(jnp.bfloat16),
            ],
            axis=1,
        )
        arrived = exchange(channel_terms.reshape(z, half, -1), "z")
        channel_summed = jnp.sum(arrived.astype(jnp.float32), axis=0)
        second_scale = lax.rsqrt(channel_summed[:, units : units + 1] / D + epsilon)
        gate_part = second_scale * channel_summed[:, :units]
        up_part = second_scale * channel_summed[:, units + pad :]
        activated = (jax.nn.silu(gate_part) * up_part).astype(jnp.bfloat16)
    with jax.named_scope("finish"):
        all_activated = exchange(copies(activated, z), "z").reshape(rows, units)
        here = (jnp.arange(rows) // half == lax.axis_index("kv"))[:, None]
        unit_terms = [
            wide_dot(all_activated, matrix) + jnp.where(here, part, 0.0)
            for matrix, part in zip((hidden_down, partner_down), middle)
        ]
        sent = jnp.stack(own_and_partner(unit_terms)).reshape(2 * kv, half, features)
        arrived = exchange(sent, ("core", "kv")).reshape(2, kv, half, features)
        return jnp.sum(arrived, axis=1).reshape(own_rows, features).astype(jnp.bfloat16)


def solution(mesh):
    kv, tp = mesh.shape["kv"], mesh.shape["tp"]
    chips = Mesh(mesh.devices.reshape(kv, tp // 2, 2), ("kv", "z", "core"))
    tp = ("z", "core")
    in_specs = (
        P("kv", tp),
        P(tp),
        P(tp, "kv"),
        P(tp, "kv"),
        P(tp, "kv"),
        P(tp, "kv"),
        P("kv"),
        P(tp, "kv", None, None),
        P(tp, "kv", None, None),
        P(tp, "kv", None, None),
        P(tp),
        P("kv"),
        P("kv", tp),
        P(tp),
        P(tp, "kv"),
        P(tp, "kv"),
        P("kv", tp),
    )
    return jax.shard_map(
        local, mesh=chips, in_specs=in_specs, out_specs=P("kv", tp), check_vma=False
    )
```

```python
import functools

import jax
import jax.numpy as jnp
from jax import lax
from jax.experimental import pallas as pl
from jax.experimental.pallas import tpu as pltpu
from jax.sharding import Mesh
from jax.sharding import PartitionSpec as P

D = 4096
LANES = 128


epsilon = 1e-06


def exchange(parts, axes):
    return lax.all_to_all(parts, axes, split_axis=0, concat_axis=0, tiled=True)


def copies(value, count):
    return jnp.broadcast_to(value, (count, *value.shape))


def from_partner(value):
    return lax.ppermute(value, "core", [(0, 1), (1, 0)])


def wide_dot(left, right):
    return jnp.dot(left, right, preferred_element_type=jnp.float32)


def as_column(value, width):
    return jnp.pad(value, ((0, 0), (0, width - 1))).astype(jnp.bfloat16)


IN_VMEM = pl.BlockSpec(memory_space=pltpu.VMEM)
IN_HBM = pl.BlockSpec(memory_space=pltpu.HBM)
GAIN_ROWS = 16


def thirds(value):
    high = value.astype(jnp.bfloat16)
    rest = value - high.astype(jnp.float32)
    middle = rest.astype(jnp.bfloat16)
    return high, middle, (rest - middle.astype(jnp.float32)).astype(jnp.bfloat16)


def gain_block(gain, width):
    row = lax.broadcasted_iota(jnp.int32, (GAIN_ROWS, width), 0)
    high, middle, low = (part.astype(jnp.float32) for part in thirds(gain))
    block = jnp.where(row == 0, high, jnp.where(row == 1, middle, jnp.where(row == 2, low, 0.0)))
    return block.astype(jnp.bfloat16)


def from_thirds(block):
    wide = block.astype(jnp.float32)
    return wide[0:1] + wide[1:2] + wide[2:3]


def join_kernel(places, *refs):
    *sources, gain, out, arrived = refs
    moves = [
        pltpu.make_async_copy(source, out.at[place], arrived.at[i])
        for i, (source, place) in enumerate(zip(sources, places))
    ]
    for move in moves:
        move.start()
    rows = out.shape[0] - GAIN_ROWS
    out[rows:, :LANES] = gain_block(gain[...], LANES)
    for move in moves:
        move.wait()


def joined(arrays, gain, axis):
    places, at = [], 0
    for array in arrays:
        span = slice(at, at + array.shape[axis])
        at += array.shape[axis]
        places.append((slice(0, array.shape[0]), span) if axis == 1 else (span,))
    shape = (arrays[0].shape[0] + GAIN_ROWS, at) if axis == 1 else (at + GAIN_ROWS, LANES)
    return pl.pallas_call(
        functools.partial(join_kernel, places),
        out_shape=pltpu.VMEM(shape, jnp.bfloat16),
        in_specs=[IN_HBM] * len(arrays) + [IN_VMEM],
        out_specs=IN_VMEM,
        scratch_shapes=[pltpu.SemaphoreType.DMA((len(arrays),))],
        compiler_params=pltpu.CompilerParams(vmem_limit_bytes=8 << 20),
        cost_estimate=pl.CostEstimate(flops=2_000_000, bytes_accessed=1_000_000, transcendentals=0),
        name="join",
    )(*(pltpu.with_memory_space_constraint(array, pltpu.HBM) for array in arrays), gain[None])


def transposed_dot(left, right):
    return lax.dot_general(
        left, right, (((1,), (1,)), ((), ())), preferred_element_type=jnp.float32
    )


def store_by_peer(terms, wide):
    half = terms.shape[1]
    for i in range(terms.shape[0]):
        terms[i] = wide[half * i : half * (i + 1)].astype(jnp.bfloat16)


def project_kernel(stream, own, partner, terms, wide):
    _, rows, features = stream.shape
    width = own.shape[1]
    parts = [stream[i].astype(jnp.float32) for i in range(2)]
    total = None
    for part, weights in zip(parts, (own, partner)):
        gain = from_thirds(weights[features : features + GAIN_ROWS, :features])
        scaled = (part * gain).astype(jnp.bfloat16)
        term = jnp.dot(scaled, weights[:features], preferred_element_type=jnp.float32)
        total = term if total is None else total + term
    wide[:, :width] = total
    squares = jnp.sum(parts[0] * parts[0] + parts[1] * parts[1], axis=1, keepdims=True)
    lane = lax.broadcasted_iota(jnp.int32, (rows, LANES), 1)
    wide[:, width:] = jnp.where(lane == 0, squares, 0.0)
    store_by_peer(terms, wide)


def project(stream, own, partner, z):
    rows = stream.shape[1]
    width = own.shape[1] + LANES
    return pl.pallas_call(
        project_kernel,
        out_shape=jax.ShapeDtypeStruct((z, rows // z, width), jnp.bfloat16),
        in_specs=[IN_VMEM] * 3,
        out_specs=IN_VMEM,
        scratch_shapes=[pltpu.VMEM((rows, width), jnp.float32)],
        compiler_params=pltpu.CompilerParams(vmem_limit_bytes=8 << 20),
        cost_estimate=pl.CostEstimate(flops=8_000_000, bytes_accessed=1_000_000, transcendentals=0),
        name="project",
    )(stream, own, partner)


def channel_kernel(
    head, units, pad, parts, stream, gain, gate, up, partner, terms, residual, wide
):
    rows, features = stream.shape[1:]
    half = terms.shape[1]
    mixer_out = parts[0].astype(jnp.float32)
    for i in range(1, parts.shape[0]):
        mixer_out = mixer_out + parts[i].astype(jnp.float32)
    own = stream[0].astype(jnp.float32) + mixer_out[:, :features]
    other = stream[1].astype(jnp.float32) + mixer_out[:, features:]
    at = head + 3 * units
    other_gain = from_thirds(partner[at : at + GAIN_ROWS])
    scaled_own = (own * gain[...]).astype(jnp.bfloat16)
    scaled_other = (other * other_gain).astype(jnp.bfloat16)
    squares = jnp.sum(own * own + other * other, axis=1, keepdims=True)
    wide[:, :units] = transposed_dot(scaled_own, gate[...]) + transposed_dot(
        scaled_other, partner[head : head + units]
    )
    lane = lax.broadcasted_iota(jnp.int32, (rows, pad), 1)
    wide[:, units : units + pad] = jnp.where(lane == 0, squares, 0.0)
    wide[:, units + pad :] = transposed_dot(scaled_own, up[...]) + transposed_dot(
        scaled_other, partner[head + units : head + 2 * units]
    )
    store_by_peer(terms, wide)
    row = lax.broadcasted_iota(jnp.int32, (rows, features), 0)
    here = row // half == lax.axis_index("kv")
    residual[0] = jnp.where(here, own, 0.0)
    residual[1] = jnp.where(here, other, 0.0)


def channel(parts, stream, gain, gate, up, partner, head, z):
    units = gate.shape[0]
    pad = -units % LANES
    _, rows, features = stream.shape
    width = 2 * units + pad
    return pl.pallas_call(
        functools.partial(channel_kernel, head, units, pad),
        out_shape=(
            jax.ShapeDtypeStruct((z, rows // z, width), jnp.bfloat16),
            jax.ShapeDtypeStruct((2, rows, features), jnp.float32),
        ),
        in_specs=[IN_VMEM] * 6,
        out_specs=(IN_VMEM, IN_VMEM),
        scratch_shapes=[pltpu.VMEM((rows, width), jnp.float32)],
        compiler_params=pltpu.CompilerParams(vmem_limit_bytes=8 << 20),
        cost_estimate=pl.CostEstimate(flops=8_000_000, bytes_accessed=1_000_000, transcendentals=0),
        name="channel",
    )(parts, stream, gain[None], gate, up, partner)


def rotate(vectors, position):
    half_dim = vectors.shape[-1] // 2
    inverse = 10000.0 ** (-jnp.arange(half_dim, dtype=jnp.float32) / half_dim)
    angles = position.astype(jnp.float32)[:, None, None] * inverse
    cosine_part = jnp.cos(angles)
    sine_part = jnp.sin(angles)
    front_half = vectors[..., :half_dim]
    back_half = vectors[..., half_dim:]
    return jnp.concatenate(
        [
            front_half * cosine_part - back_half * sine_part,
            front_half * sine_part + back_half * cosine_part,
        ],
        axis=-1,
    )


def retain(
    queries,
    keys_new,
    values_new,
    gates,
    decay_rate,
    prior_state,
    key_block,
    value_block,
    lengths,
    group_gain,
):
    batch_rows = queries.shape[0]
    heads_here = decay_rate.shape[0]
    key_width = prior_state.shape[2]
    value_width = prior_state.shape[3]
    block_len = key_block.shape[2]
    rotated = rotate(
        queries.astype(jnp.float32).reshape(batch_rows, heads_here, key_width), lengths
    ).astype(jnp.bfloat16)
    fresh_keys = rotate(
        keys_new.astype(jnp.float32).reshape(batch_rows, heads_here, key_width), lengths
    ) * key_width ** (-0.5)
    fresh_values = values_new.astype(jnp.float32).reshape(batch_rows, heads_here, value_width)
    filled = lengths % block_len
    slots = jnp.arange(block_len, dtype=jnp.int32)
    distance = (filled[:, None] - slots[None, :]).astype(jnp.float32)
    live_slots = (slots[None, :] < filled[:, None])[:, None, :]
    weighting = jnp.where(
        live_slots, jnp.exp(-decay_rate[None, :, None] * distance[:, None, :]), jnp.float32(0.0)
    )
    scores = jnp.einsum("shk,shjk->shj", rotated, key_block, preferred_element_type=jnp.float32)
    block_weights = (scores * weighting).astype(jnp.bfloat16)
    block_term = jnp.einsum(
        "shj,shjv->shv", block_weights, value_block, preferred_element_type=jnp.float32
    )
    rotated_wide = rotated.astype(jnp.float32)
    own_term = jnp.sum(rotated_wide * fresh_keys, axis=-1, keepdims=True) * fresh_values
    carried = jnp.exp(-decay_rate[None, :, None] * (filled[:, None, None] + 1).astype(jnp.float32))
    state_term = carried * jnp.einsum(
        "shk,shkv->shv", rotated_wide, prior_state, precision=lax.Precision.HIGHEST
    )
    retained = own_term + block_term + state_term
    centre = jnp.mean(retained, axis=-1, keepdims=True)
    spread = jnp.mean(jnp.square(retained - centre), axis=-1, keepdims=True)
    normed = (retained - centre) * lax.rsqrt(spread + epsilon)
    gated = (
        jax.nn.silu(gates.astype(jnp.float32)).reshape(batch_rows, heads_here, value_width)
        * normed
        * group_gain.reshape(heads_here, value_width)
    )
    return gated.astype(jnp.bfloat16).reshape(batch_rows, heads_here * value_width)


def local(
    hidden_in,
    mixer_gain,
    query_weight,
    key_weight,
    value_weight,
    gate_weight,
    decay_rate,
    prior_state,
    key_block,
    value_block,
    lengths,
    group_gain,
    output_weight,
    channel_gain,
    hidden_gate,
    hidden_up,
    hidden_down,
):
    kv, z = lax.axis_size("kv"), lax.axis_size("z")
    core = lax.axis_index("core")
    own_rows, features = hidden_in.shape
    half = own_rows // 2
    rows = kv * half
    key_width, value_width = query_weight.shape[1], value_weight.shape[1]
    head_width, units = output_weight.shape[0], hidden_gate.shape[1]
    pad = -units % LANES

    def own_and_partner(pair):
        swapped = core == 1
        return (
            jnp.where(swapped, pair[1], pair[0]),
            jnp.where(swapped, pair[0], pair[1]),
        )

    with jax.named_scope("rows"):
        sent = copies(hidden_in, 2 * kv)
        arrived = exchange(sent, ("core", "kv")).reshape(2, kv, 2, half, features)
        mine = jnp.where(core == 1, arrived[:, :, 1], arrived[:, :, 0])
        stream = jnp.stack(own_and_partner(mine.reshape(2, rows, features)))
    with jax.named_scope("swap_first"):
        first_own = joined((query_weight, key_weight, value_weight, gate_weight), mixer_gain, 1)
        first_partner = from_partner(first_own)
    with jax.named_scope("swap_second"):
        later = (output_weight, hidden_gate.T, hidden_up.T, hidden_down)
        later, stream = lax.optimization_barrier((later, stream))
        second_partner = from_partner(joined(later, channel_gain, 0))
        partner_output = second_partner[:head_width]
        partner_down = second_partner[head_width + 2 * units : head_width + 3 * units]

    with jax.named_scope("project"):
        arrived = exchange(project(stream, first_own, first_partner, z), "z")
        summed = jnp.sum(arrived.astype(jnp.float32), axis=0)
    with jax.named_scope("retain"):
        ends = [key_width, 2 * key_width, 2 * key_width + value_width]
        ends.append(ends[-1] + value_width)
        *projected, row_squares = jnp.split(summed, ends, axis=1)
        first_scale = lax.rsqrt(row_squares[:, :1] / D + epsilon)
        projected = [(first_scale * part).astype(jnp.bfloat16) for part in projected]
        mixed = retain(
            *projected,
            decay_rate,
            prior_state,
            key_block,
            value_block,
            lengths,
            group_gain,
        )
    with jax.named_scope("mix"):
        all_mixed = exchange(copies(mixed, z), "z").reshape(rows, head_width)
        head_terms = jnp.concatenate(
            [wide_dot(all_mixed, output_weight), wide_dot(all_mixed, partner_output)], axis=1
        ).astype(jnp.bfloat16)
        head_parts = exchange(copies(head_terms, kv), "kv")
    with jax.named_scope("channel"):
        channel_terms, residual = channel(
            head_parts,
            stream,
            channel_gain,
            hidden_gate.T,
            hidden_up.T,
            second_partner,
            head_width,
            z,
        )
        arrived = exchange(channel_terms, "z")
        channel_summed = jnp.sum(arrived.astype(jnp.float32), axis=0)
        second_scale = lax.rsqrt(channel_summed[:, units : units + 1] / D + epsilon)
        gate_part = second_scale * channel_summed[:, :units]
        up_part = second_scale * channel_summed[:, units + pad :]
        activated = (jax.nn.silu(gate_part) * up_part).astype(jnp.bfloat16)
    with jax.named_scope("finish"):
        all_activated = exchange(copies(activated, z), "z").reshape(rows, units)
        unit_terms = [
            wide_dot(all_activated, matrix) + part
            for matrix, part in zip((hidden_down, partner_down), residual)
        ]
        sent = jnp.stack(own_and_partner(unit_terms)).reshape(2 * kv, half, features)
        arrived = exchange(sent, ("core", "kv")).reshape(2, kv, half, features)
        return jnp.sum(arrived, axis=1).reshape(own_rows, features).astype(jnp.bfloat16)


def solution(mesh):
    kv, tp = mesh.shape["kv"], mesh.shape["tp"]
    chips = Mesh(mesh.devices.reshape(kv, tp // 2, 2), ("kv", "z", "core"))
    tp = ("z", "core")
    in_specs = (
        P("kv", tp),
        P(tp),
        P(tp, "kv"),
        P(tp, "kv"),
        P(tp, "kv"),
        P(tp, "kv"),
        P("kv"),
        P(tp, "kv", None, None),
        P(tp, "kv", None, None),
        P(tp, "kv", None, None),
        P(tp),
        P("kv"),
        P("kv", tp),
        P(tp),
        P(tp, "kv"),
        P(tp, "kv"),
        P("kv", tp),
    )
    return jax.shard_map(
        local, mesh=chips, in_specs=in_specs, out_specs=P("kv", tp), check_vma=False
    )
```

```python
import functools

import jax
import jax.numpy as jnp
from jax import lax
from jax.experimental import pallas as pl
from jax.experimental.pallas import tpu as pltpu
from jax.sharding import Mesh
from jax.sharding import PartitionSpec as P

D = 4096
LANES = 128
BLOCK = 128


epsilon = 1e-06


def exchange(parts, axes):
    return lax.all_to_all(parts, axes, split_axis=0, concat_axis=0, tiled=True)


def copies(value, count):
    return jnp.broadcast_to(value, (count, *value.shape))


def from_partner(value):
    return lax.ppermute(value, "core", [(0, 1), (1, 0)])


def wide_dot(left, right):
    return jnp.dot(left, right, preferred_element_type=jnp.float32)


IN_VMEM = pl.BlockSpec(memory_space=pltpu.VMEM)
IN_HBM = pl.BlockSpec(memory_space=pltpu.HBM)
GAIN_ROWS = 16


def thirds(value):
    high = value.astype(jnp.bfloat16)
    rest = value - high.astype(jnp.float32)
    middle = rest.astype(jnp.bfloat16)
    return high, middle, (rest - middle.astype(jnp.float32)).astype(jnp.bfloat16)


def from_thirds(block):
    wide = block.astype(jnp.float32)
    return wide[0:1] + wide[1:2] + wide[2:3]


def open_kernel(
    first_at,
    second_at,
    hidden,
    lengths,
    mixer_gain,
    channel_gain,
    inverse,
    *refs,
):
    count = len(first_at) + len(second_at)
    sources = refs[:count]
    sent, first, second, table, rows, many, gains, place, arrived = refs[count:]
    moves = [
        pltpu.make_async_copy(source, target, arrived.at[i])
        for i, (source, target) in enumerate(
            [
                (hidden, rows),
                (lengths, place),
                (mixer_gain, gains.at[0:1]),
                (channel_gain, gains.at[1:2]),
                *((source, first.at[at]) for source, at in zip(sources, first_at)),
                *((source, second.at[at]) for source, at in zip(sources[len(first_at) :], second_at)),
            ]
        )
    ]
    for move in moves:
        move.start()
    lane = lax.broadcasted_iota(jnp.int32, (1, LANES), 1)
    moves[0].wait()
    many[...] = jnp.broadcast_to(rows[...][None], many.shape)
    out = pltpu.make_async_copy(many, sent, arrived.at[len(moves)])
    out.start()
    moves[1].wait()
    seqs = place.shape[0]
    for i in range(seqs):
        angle = place[i].astype(jnp.float32) * inverse[...]
        filled = lax.rem(place[i], BLOCK)
        table[i : i + 1] = jnp.cos(angle)
        table[seqs + i : seqs + i + 1] = jnp.sin(angle)
        table[2 * seqs + i : 2 * seqs + i + 1] = (filled - lane).astype(jnp.float32)
        table[3 * seqs + i : 3 * seqs + i + 1] = (filled + 1 + 0 * lane).astype(jnp.float32)
    moves[2].wait()
    moves[3].wait()
    for target, gain in zip((first, second), (gains[0:1], gains[1:2])):
        high, middle, low = (part.astype(jnp.float32) for part in thirds(gain))
        row = lax.broadcasted_iota(jnp.int32, (GAIN_ROWS, LANES), 0)
        block = jnp.where(row == 0, high, jnp.where(row == 1, middle, jnp.where(row == 2, low, 0.0)))
        target[target.shape[0] - GAIN_ROWS :, :LANES] = block.astype(jnp.bfloat16)
    for move in moves[4:]:
        move.wait()
    out.wait()


def opening(hidden, lengths, mixer_gain, channel_gain, first, second, peers):
    half = LANES
    inverse = 10000.0 ** (-jnp.arange(half, dtype=jnp.float32) / half)
    first_at, at = [], 0
    for array in first:
        first_at.append((slice(0, array.shape[0]), slice(at, at + array.shape[1])))
        at += array.shape[1]
    first_shape = (first[0].shape[0] + GAIN_ROWS, at)
    second_at, at = [], 0
    for array in second:
        second_at.append((slice(at, at + array.shape[0]),))
        at += array.shape[0]
    second_shape = (at + GAIN_ROWS, LANES)
    in_hbm = [hidden, lengths, mixer_gain[None], channel_gain[None]]
    in_hbm = [pltpu.with_memory_space_constraint(array, pltpu.HBM) for array in in_hbm]
    weights = [
        pltpu.with_memory_space_constraint(array, pltpu.HBM) for array in (*first, *second)
    ]
    many = (peers, *hidden.shape)
    return pl.pallas_call(
        functools.partial(open_kernel, first_at, second_at),
        out_shape=(
            jax.ShapeDtypeStruct(many, jnp.bfloat16),
            pltpu.VMEM(first_shape, jnp.bfloat16),
            pltpu.VMEM(second_shape, jnp.bfloat16),
            pltpu.VMEM((4 * lengths.shape[0], LANES), jnp.float32),
        ),
        in_specs=[IN_HBM] * 4 + [IN_VMEM] + [IN_HBM] * len(weights),
        out_specs=(IN_HBM, IN_VMEM, IN_VMEM, IN_VMEM),
        scratch_shapes=[
            pltpu.VMEM(hidden.shape, jnp.bfloat16),
            pltpu.VMEM(many, jnp.bfloat16),
            pltpu.VMEM((2, LANES), jnp.float32),
            pltpu.SMEM(lengths.shape, jnp.int32),
            pltpu.SemaphoreType.DMA((5 + len(weights),)),
        ],
        compiler_params=pltpu.CompilerParams(vmem_limit_bytes=8 << 20),
        cost_estimate=pl.CostEstimate(flops=2_000_000, bytes_accessed=1_000_000, transcendentals=0),
        name="opening",
    )(*in_hbm, inverse[None], *weights)


def rotated_by(vectors, cosine, sine):
    half = cosine.shape[1]
    front, back = vectors[:, :half], vectors[:, half:]
    return jnp.concatenate([front * cosine - back * sine, front * sine + back * cosine], axis=1)


def of_each(row, products):
    result = products[0]
    for i, product in enumerate(products[1:], 1):
        result = jnp.where(row == i, product, result)
    return result


def retain_kernel(decay, arrived, table, state, keys, values, group_gain, mixed):
    seqs, _, key_width, value_width = state.shape
    total = arrived[0].astype(jnp.float32)
    for i in range(1, arrived.shape[0]):
        total = total + arrived[i].astype(jnp.float32)
    ends = 2 * (key_width + value_width)
    scale = lax.rsqrt(total[:, ends : ends + 1] / D + epsilon)
    ready = (scale * total[:, :ends]).astype(jnp.bfloat16).astype(jnp.float32)
    cosine, sine = table[:seqs], table[seqs : 2 * seqs]
    distance = table[2 * seqs : 3 * seqs]
    weighting = jnp.where(distance > 0.0, jnp.exp(-decay[0] * distance), 0.0)
    carried = jnp.exp(-decay[0] * table[3 * seqs :, :1])
    query = rotated_by(ready[:, :key_width], cosine, sine).astype(jnp.bfloat16)
    fresh = rotated_by(ready[:, key_width : 2 * key_width], cosine, sine) * key_width ** (-0.5)
    value = ready[:, 2 * key_width : 2 * key_width + value_width]
    gate = ready[:, 2 * key_width + value_width :]
    own = jnp.sum(query.astype(jnp.float32) * fresh, axis=1, keepdims=True) * value
    row_k = lax.broadcasted_iota(jnp.int32, (seqs, keys.shape[2]), 0)
    row_v = lax.broadcasted_iota(jnp.int32, (seqs, value_width), 0)
    scores = of_each(row_k, [transposed_dot(query, keys[i, 0]) for i in range(seqs)])
    block_weights = (scores * weighting).astype(jnp.bfloat16)
    block = of_each(row_v, [wide_dot(block_weights, values[i, 0]) for i in range(seqs)])
    remembered = []
    for i in range(seqs):
        high = state[i, 0].astype(jnp.bfloat16)
        low = (state[i, 0] - high.astype(jnp.float32)).astype(jnp.bfloat16)
        remembered.append(wide_dot(query, high) + wide_dot(query, low))
    retained = own + block + carried * of_each(row_v, remembered)
    centre = jnp.mean(retained, axis=1, keepdims=True)
    away = retained - centre
    spread = jnp.mean(away * away, axis=1, keepdims=True)
    normed = away * lax.rsqrt(spread + epsilon)
    result = (jax.nn.silu(gate) * normed * group_gain[...]).astype(jnp.bfloat16)
    for i in range(mixed.shape[0]):
        mixed[i] = result


def retain(decay, arrived, table, state, keys, values, group_gain):
    z = arrived.shape[0]
    seqs, _, _, value_width = state.shape
    return pl.pallas_call(
        retain_kernel,
        out_shape=jax.ShapeDtypeStruct((z, seqs, value_width), jnp.bfloat16),
        in_specs=[pl.BlockSpec(memory_space=pltpu.SMEM)] + [IN_VMEM] * 6,
        out_specs=IN_VMEM,
        compiler_params=pltpu.CompilerParams(vmem_limit_bytes=8 << 20),
        cost_estimate=pl.CostEstimate(flops=8_000_000, bytes_accessed=2_000_000, transcendentals=0),
        name="retain",
    )(decay, arrived, table, state, keys, values, group_gain[None])


def activate_kernel(units, pad, arrived, activated):
    total = arrived[0].astype(jnp.float32)
    for i in range(1, arrived.shape[0]):
        total = total + arrived[i].astype(jnp.float32)
    scale = lax.rsqrt(total[:, units : units + 1] / D + epsilon)
    gate, up = scale * total[:, :units], scale * total[:, units + pad :]
    result = (jax.nn.silu(gate) * up).astype(jnp.bfloat16)
    for i in range(activated.shape[0]):
        activated[i] = result


def activate(arrived, units, pad):
    z, half, _ = arrived.shape
    return pl.pallas_call(
        functools.partial(activate_kernel, units, pad),
        out_shape=jax.ShapeDtypeStruct((z, half, units), jnp.bfloat16),
        in_specs=[IN_VMEM],
        out_specs=IN_VMEM,
        compiler_params=pltpu.CompilerParams(vmem_limit_bytes=8 << 20),
        cost_estimate=pl.CostEstimate(flops=1_000_000, bytes_accessed=200_000, transcendentals=0),
        name="activate",
    )(arrived)


def transposed_dot(left, right):
    return lax.dot_general(
        left, right, (((1,), (1,)), ((), ())), preferred_element_type=jnp.float32
    )


def store_by_peer(terms, wide):
    half = terms.shape[1]
    for i in range(terms.shape[0]):
        terms[i] = wide[half * i : half * (i + 1)].astype(jnp.bfloat16)


def project_kernel(stream, own, partner, terms, wide):
    _, rows, features = stream.shape
    width = own.shape[1]
    parts = [stream[i].astype(jnp.float32) for i in range(2)]
    total = None
    for part, weights in zip(parts, (own, partner)):
        gain = from_thirds(weights[features : features + GAIN_ROWS, :features])
        scaled = (part * gain).astype(jnp.bfloat16)
        term = jnp.dot(scaled, weights[:features], preferred_element_type=jnp.float32)
        total = term if total is None else total + term
    wide[:, :width] = total
    squares = jnp.sum(parts[0] * parts[0] + parts[1] * parts[1], axis=1, keepdims=True)
    lane = lax.broadcasted_iota(jnp.int32, (rows, LANES), 1)
    wide[:, width:] = jnp.where(lane == 0, squares, 0.0)
    store_by_peer(terms, wide)


def project(stream, own, partner, z):
    rows = stream.shape[1]
    width = own.shape[1] + LANES
    return pl.pallas_call(
        project_kernel,
        out_shape=jax.ShapeDtypeStruct((z, rows // z, width), jnp.bfloat16),
        in_specs=[IN_VMEM] * 3,
        out_specs=IN_VMEM,
        scratch_shapes=[pltpu.VMEM((rows, width), jnp.float32)],
        compiler_params=pltpu.CompilerParams(vmem_limit_bytes=8 << 20),
        cost_estimate=pl.CostEstimate(flops=8_000_000, bytes_accessed=1_000_000, transcendentals=0),
        name="project",
    )(stream, own, partner)


def channel_kernel(
    head, units, pad, parts, stream, own_weights, partner, terms, residual, wide
):
    rows, features = stream.shape[1:]
    half = terms.shape[1]
    mixer_out = parts[0].astype(jnp.float32)
    for i in range(1, parts.shape[0]):
        mixer_out = mixer_out + parts[i].astype(jnp.float32)
    own = stream[0].astype(jnp.float32) + mixer_out[:, :features]
    other = stream[1].astype(jnp.float32) + mixer_out[:, features:]
    at = head + 3 * units
    scaled_own, scaled_other = (
        (part * from_thirds(weights[at : at + GAIN_ROWS])).astype(jnp.bfloat16)
        for part, weights in ((own, own_weights), (other, partner))
    )
    squares = jnp.sum(own * own + other * other, axis=1, keepdims=True)
    wide[:, :units] = transposed_dot(
        scaled_own, own_weights[head : head + units]
    ) + transposed_dot(
        scaled_other, partner[head : head + units]
    )
    lane = lax.broadcasted_iota(jnp.int32, (rows, pad), 1)
    wide[:, units : units + pad] = jnp.where(lane == 0, squares, 0.0)
    wide[:, units + pad :] = transposed_dot(
        scaled_own, own_weights[head + units : head + 2 * units]
    ) + transposed_dot(
        scaled_other, partner[head + units : head + 2 * units]
    )
    store_by_peer(terms, wide)
    row = lax.broadcasted_iota(jnp.int32, (rows, features), 0)
    here = row // half == lax.axis_index("kv")
    residual[0] = jnp.where(here, own, 0.0)
    residual[1] = jnp.where(here, other, 0.0)


def channel(parts, stream, own_weights, partner, head, units, z):
    pad = -units % LANES
    _, rows, features = stream.shape
    width = 2 * units + pad
    return pl.pallas_call(
        functools.partial(channel_kernel, head, units, pad),
        out_shape=(
            jax.ShapeDtypeStruct((z, rows // z, width), jnp.bfloat16),
            jax.ShapeDtypeStruct((2, rows, features), jnp.float32),
        ),
        in_specs=[IN_VMEM] * 4,
        out_specs=(IN_VMEM, IN_VMEM),
        scratch_shapes=[pltpu.VMEM((rows, width), jnp.float32)],
        compiler_params=pltpu.CompilerParams(vmem_limit_bytes=8 << 20),
        cost_estimate=pl.CostEstimate(flops=8_000_000, bytes_accessed=1_000_000, transcendentals=0),
        name="channel",
    )(parts, stream, own_weights, partner)


def local(
    hidden_in,
    mixer_gain,
    query_weight,
    key_weight,
    value_weight,
    gate_weight,
    decay_rate,
    prior_state,
    key_block,
    value_block,
    lengths,
    group_gain,
    output_weight,
    channel_gain,
    hidden_gate,
    hidden_up,
    hidden_down,
):
    kv, z = lax.axis_size("kv"), lax.axis_size("z")
    core = lax.axis_index("core")
    own_rows, features = hidden_in.shape
    half = own_rows // 2
    rows = kv * half
    head_width, units = output_weight.shape[0], hidden_gate.shape[1]
    pad = -units % LANES

    def own_and_partner(pair):
        swapped = core == 1
        return (
            jnp.where(swapped, pair[1], pair[0]),
            jnp.where(swapped, pair[0], pair[1]),
        )

    with jax.named_scope("rows"):
        sent, first_own, second_own, table = opening(
            hidden_in,
            lengths,
            mixer_gain,
            channel_gain,
            (query_weight, key_weight, value_weight, gate_weight),
            (output_weight, hidden_gate.T, hidden_up.T, hidden_down),
            2 * kv,
        )
        arrived = exchange(sent, ("core", "kv")).reshape(2, kv, 2, half, features)
        mine = jnp.where(core == 1, arrived[:, :, 1], arrived[:, :, 0])
        stream = jnp.stack(own_and_partner(mine.reshape(2, rows, features)))
    with jax.named_scope("swap"):
        first_partner = from_partner(first_own)
        second_own, stream = lax.optimization_barrier((second_own, stream))
        second_partner = from_partner(second_own)
        own_output, partner_output = (
            weights[:head_width] for weights in (second_own, second_partner)
        )
        own_down, partner_down = (
            weights[head_width + 2 * units : head_width + 3 * units]
            for weights in (second_own, second_partner)
        )
    with jax.named_scope("project"):
        arrived = exchange(project(stream, first_own, first_partner, z), "z")
    with jax.named_scope("retain"):
        mixed = retain(
            decay_rate, arrived, table, prior_state, key_block, value_block, group_gain
        )
    with jax.named_scope("mix"):
        all_mixed = exchange(mixed, "z").reshape(rows, head_width)
        head_terms = jnp.concatenate(
            [wide_dot(all_mixed, own_output), wide_dot(all_mixed, partner_output)], axis=1
        ).astype(jnp.bfloat16)
        head_parts = exchange(copies(head_terms, kv), "kv")
    with jax.named_scope("channel"):
        channel_terms, residual = channel(
            head_parts, stream, second_own, second_partner, head_width, units, z
        )
        activated = activate(exchange(channel_terms, "z"), units, pad)
    with jax.named_scope("finish"):
        all_activated = exchange(activated, "z").reshape(rows, units)
        unit_terms = [
            wide_dot(all_activated, matrix) + part
            for matrix, part in zip((own_down, partner_down), residual)
        ]
        sent = jnp.stack(own_and_partner(unit_terms)).reshape(2 * kv, half, features)
        arrived = exchange(sent, ("core", "kv")).reshape(2, kv, half, features)
        return jnp.sum(arrived, axis=1).reshape(own_rows, features).astype(jnp.bfloat16)


def solution(mesh):
    kv, tp = mesh.shape["kv"], mesh.shape["tp"]
    chips = Mesh(mesh.devices.reshape(kv, tp // 2, 2), ("kv", "z", "core"))
    tp = ("z", "core")
    in_specs = (
        P("kv", tp),
        P(tp),
        P(tp, "kv"),
        P(tp, "kv"),
        P(tp, "kv"),
        P(tp, "kv"),
        P("kv"),
        P(tp, "kv", None, None),
        P(tp, "kv", None, None),
        P(tp, "kv", None, None),
        P(tp),
        P("kv"),
        P("kv", tp),
        P(tp),
        P(tp, "kv"),
        P(tp, "kv"),
        P("kv", tp),
    )
    return jax.shard_map(
        local, mesh=chips, in_specs=in_specs, out_specs=P("kv", tp), check_vma=False
    )
```

```python
import functools

import jax
import jax.numpy as jnp
from jax import lax
from jax.experimental import pallas as pl
from jax.experimental.pallas import tpu as pltpu
from jax.sharding import Mesh
from jax.sharding import PartitionSpec as P

D = 4096
LANES = 128
BLOCK = 128


epsilon = 1e-06


def exchange(parts, axes):
    return lax.all_to_all(parts, axes, split_axis=0, concat_axis=0, tiled=True)


def wide_dot(left, right):
    return jnp.dot(left, right, preferred_element_type=jnp.float32)


IN_VMEM = pl.BlockSpec(memory_space=pltpu.VMEM)
IN_HBM = pl.BlockSpec(memory_space=pltpu.HBM)
IN_SMEM = pl.BlockSpec(memory_space=pltpu.SMEM)
GAIN_ROWS = 16


def thirds(value):
    high = value.astype(jnp.bfloat16)
    rest = value - high.astype(jnp.float32)
    middle = rest.astype(jnp.bfloat16)
    return high, middle, (rest - middle.astype(jnp.float32)).astype(jnp.bfloat16)


def from_thirds(block):
    wide = block.astype(jnp.float32)
    return wide[0:1] + wide[1:2] + wide[2:3]


def open_kernel(at, decay, hidden, lengths, mixer_gain, channel_gain, inverse, *refs):
    sources = refs[: len(at)]
    sent, joined, table, rows, gains, place, arrived = refs[len(at) :]
    pairs = [
        (hidden, rows),
        (lengths, place),
        (mixer_gain, gains.at[0:1]),
        (channel_gain, gains.at[1:2]),
    ]
    for source, first in zip(sources, at):
        for lanes in range(0, source.shape[1], LANES):
            span = slice(first + lanes // LANES * source.shape[0], None)
            span = slice(span.start, span.start + source.shape[0])
            pairs.append((source.at[:, lanes : lanes + LANES], joined.at[span]))
    moves = [
        pltpu.make_async_copy(source, target, arrived.at[i])
        for i, (source, target) in enumerate(pairs)
    ]
    for move in moves:
        move.start()
    lane = lax.broadcasted_iota(jnp.int32, (1, LANES), 1)
    for move in moves[:4]:
        move.wait()
    peers, half, _ = sent.shape
    wide = rows[...].astype(jnp.float32)
    for i in range(peers):
        first = half * (2 * i // peers)
        sent[i] = wide[first : first + half].astype(jnp.bfloat16)
    seqs = place.shape[0]
    for i in range(seqs):
        angle = place[i].astype(jnp.float32) * inverse[...]
        filled = lax.rem(place[i], BLOCK)
        distance = (filled - lane).astype(jnp.float32)
        table[i : i + 1] = jnp.cos(angle)
        table[seqs + i : seqs + i + 1] = jnp.sin(angle)
        table[2 * seqs + i : 2 * seqs + i + 1] = jnp.where(
            lane < filled, jnp.exp(-decay[0] * distance), 0.0
        )
        reach = (filled + 1 + 0 * lane).astype(jnp.float32)
        table[3 * seqs + i : 3 * seqs + i + 1] = jnp.exp(-decay[0] * reach)
    row = lax.broadcasted_iota(jnp.int32, (GAIN_ROWS, LANES), 0)
    end = joined.shape[0]
    for i in range(2):
        high, middle, low = (part.astype(jnp.float32) for part in thirds(gains[i : i + 1]))
        block = jnp.where(row == 0, high, jnp.where(row == 1, middle, jnp.where(row == 2, low, 0.0)))
        first = end - (2 - i) * GAIN_ROWS
        joined[first : first + GAIN_ROWS] = block.astype(jnp.bfloat16)
    for move in moves[4:]:
        move.wait()


def opening(hidden, lengths, decay, mixer_gain, channel_gain, weights, peers):
    inverse = 10000.0 ** (-jnp.arange(LANES, dtype=jnp.float32) / LANES)
    at, end = [], 0
    for array in weights:
        at.append(end)
        end += array.size // LANES
    in_hbm = [
        pltpu.with_memory_space_constraint(array, pltpu.HBM)
        for array in (hidden, lengths, mixer_gain[None], channel_gain[None], *weights)
    ]
    pieces = sum(array.shape[1] // LANES for array in weights)
    return pl.pallas_call(
        functools.partial(open_kernel, at),
        out_shape=(
            jax.ShapeDtypeStruct((peers, hidden.shape[0] // 2, LANES), jnp.bfloat16),
            pltpu.VMEM((end + 2 * GAIN_ROWS, LANES), jnp.bfloat16),
            pltpu.VMEM((4 * lengths.shape[0], LANES), jnp.float32),
        ),
        in_specs=[IN_SMEM] + [IN_HBM] * 4 + [IN_VMEM] + [IN_HBM] * len(weights),
        out_specs=(IN_VMEM, IN_VMEM, IN_VMEM),
        scratch_shapes=[
            pltpu.VMEM(hidden.shape, jnp.bfloat16),
            pltpu.VMEM((2, LANES), jnp.float32),
            pltpu.SMEM(lengths.shape, jnp.int32),
            pltpu.SemaphoreType.DMA((4 + pieces,)),
        ],
        compiler_params=pltpu.CompilerParams(vmem_limit_bytes=8 << 20),
        cost_estimate=pl.CostEstimate(flops=2_000_000, bytes_accessed=1_000_000, transcendentals=0),
        name="opening",
    )(decay, *in_hbm[:4], inverse[None], *in_hbm[4:])


def rotated_by(vectors, cosine, sine):
    half = cosine.shape[1]
    front, back = vectors[:, :half], vectors[:, half:]
    return jnp.concatenate([front * cosine - back * sine, front * sine + back * cosine], axis=1)


def of_each(row, products):
    result = products[0]
    for i, product in enumerate(products[1:], 1):
        result = jnp.where(row == i, product, result)
    return result


def retain_kernel(arrived, table, state, keys, values, group_gain, mixed):
    seqs, _, key_width, value_width = state.shape
    total = arrived[0].astype(jnp.float32)
    for i in range(1, arrived.shape[0]):
        total = total + arrived[i].astype(jnp.float32)
    ends = 2 * (key_width + value_width)
    scale = lax.rsqrt(total[:, ends : ends + 1] / D + epsilon)
    ready = (scale * total[:, :ends]).astype(jnp.bfloat16).astype(jnp.float32)
    cosine, sine = table[:seqs], table[seqs : 2 * seqs]
    weighting = table[2 * seqs : 3 * seqs]
    carried = table[3 * seqs :, :1]
    query = rotated_by(ready[:, :key_width], cosine, sine).astype(jnp.bfloat16)
    fresh = rotated_by(ready[:, key_width : 2 * key_width], cosine, sine) * key_width ** (-0.5)
    value = ready[:, 2 * key_width : 2 * key_width + value_width]
    gate = ready[:, 2 * key_width + value_width :]
    own = jnp.sum(query.astype(jnp.float32) * fresh, axis=1, keepdims=True) * value
    row_k = lax.broadcasted_iota(jnp.int32, (seqs, keys.shape[2]), 0)
    row_v = lax.broadcasted_iota(jnp.int32, (seqs, value_width), 0)
    scores = of_each(row_k, [transposed_dot(query, keys[i, 0]) for i in range(seqs)])
    block_weights = (scores * weighting).astype(jnp.bfloat16)
    block = of_each(row_v, [wide_dot(block_weights, values[i, 0]) for i in range(seqs)])
    remembered = []
    for i in range(seqs):
        high = state[i, 0].astype(jnp.bfloat16)
        low = (state[i, 0] - high.astype(jnp.float32)).astype(jnp.bfloat16)
        remembered.append(wide_dot(query, high) + wide_dot(query, low))
    retained = own + block + carried * of_each(row_v, remembered)
    centre = jnp.mean(retained, axis=1, keepdims=True)
    away = retained - centre
    spread = jnp.mean(away * away, axis=1, keepdims=True)
    normed = away * lax.rsqrt(spread + epsilon)
    result = (jax.nn.silu(gate) * normed * group_gain[...]).astype(jnp.bfloat16)
    for i in range(mixed.shape[0]):
        mixed[i] = result


def retain(arrived, table, state, keys, values, group_gain):
    seqs, _, _, value_width = state.shape
    out_shape = jax.ShapeDtypeStruct((arrived.shape[0], seqs, value_width), jnp.bfloat16)
    operands = (arrived, table, state, keys, values, group_gain[None])
    return call(retain_kernel, out_shape, operands, [], "retain")


def activate_kernel(units, pad, arrived, activated):
    total = arrived[0].astype(jnp.float32)
    for i in range(1, arrived.shape[0]):
        total = total + arrived[i].astype(jnp.float32)
    scale = lax.rsqrt(total[:, units : units + 1] / D + epsilon)
    gate, up = scale * total[:, :units], scale * total[:, units + pad :]
    result = (jax.nn.silu(gate) * up).astype(jnp.bfloat16)
    for i in range(activated.shape[0]):
        activated[i] = result


def activate(arrived, units, pad):
    out_shape = jax.ShapeDtypeStruct((*arrived.shape[:2], units), jnp.bfloat16)
    kernel = functools.partial(activate_kernel, units, pad)
    return call(kernel, out_shape, (arrived,), [], "activate")


def transposed_dot(left, right):
    return lax.dot_general(
        left, right, (((1,), (1,)), ((), ())), preferred_element_type=jnp.float32
    )


def store_by_peer(terms, wide):
    half = terms.shape[1]
    for i in range(terms.shape[0]):
        terms[i] = wide[half * i : half * (i + 1)].astype(jnp.bfloat16)


def gathered_rows(arrived, wide):
    half = arrived.shape[1]
    for i in range(arrived.shape[0]):
        wide[half * i : half * (i + 1)] = arrived[i].astype(jnp.float32)


def project_kernel(arrived, own, partner, terms, stream, wide):
    _, rows, features = stream.shape
    half = terms.shape[1]
    width = wide.shape[1] - LANES
    side = lax.axis_index("core")
    for i in range(rows // half):
        span = slice(half * i, half * (i + 1))
        stream[0, span] = arrived[side, i].astype(jnp.float32)
        stream[1, span] = arrived[1 - side, i].astype(jnp.float32)
    parts = [stream[i] for i in range(2)]
    end = own.shape[0]
    scaled = jnp.concatenate(
        [
            (part * from_thirds(weights[end - 2 * GAIN_ROWS : end - GAIN_ROWS])).astype(
                jnp.bfloat16
            )
            for part, weights in zip(parts, (own, partner))
        ],
        axis=1,
    )
    for i in range(width // LANES):
        span = slice(features * i, features * (i + 1))
        columns = jnp.concatenate([own[span], partner[span]], axis=0)
        wide[:, LANES * i : LANES * (i + 1)] = wide_dot(scaled, columns)
    squares = jnp.sum(parts[0] * parts[0] + parts[1] * parts[1], axis=1, keepdims=True)
    lane = lax.broadcasted_iota(jnp.int32, (rows, LANES), 1)
    wide[:, width:] = jnp.where(lane == 0, squares, 0.0)
    store_by_peer(terms, wide)


def call(kernel, out_shape, operands, scratch, name):
    return pl.pallas_call(
        kernel,
        out_shape=out_shape,
        in_specs=[IN_VMEM] * len(operands),
        out_specs=jax.tree.map(lambda _: IN_VMEM, out_shape),
        scratch_shapes=scratch,
        compiler_params=pltpu.CompilerParams(vmem_limit_bytes=8 << 20),
        cost_estimate=pl.CostEstimate(flops=8_000_000, bytes_accessed=1_000_000, transcendentals=0),
        name=name,
    )(*operands)


def project(arrived, own, partner, width, z):
    _, kv, half, features = arrived.shape
    rows = kv * half
    width = width + LANES
    out_shape = (
        jax.ShapeDtypeStruct((z, rows // z, width), jnp.bfloat16),
        jax.ShapeDtypeStruct((2, rows, features), jnp.float32),
    )
    scratch = [pltpu.VMEM((rows, width), jnp.float32)]
    return call(project_kernel, out_shape, (arrived, own, partner), scratch, "project")


def mix_kernel(head, arrived, own, partner, terms, wide):
    gathered_rows(arrived, wide)
    every = wide[...].astype(jnp.bfloat16)
    span = slice(head, head + wide.shape[1])
    both = jnp.concatenate([wide_dot(every, own[span]), wide_dot(every, partner[span])], axis=1)
    both = both.astype(jnp.bfloat16)
    for i in range(terms.shape[0]):
        terms[i] = both


def mix(arrived, own, partner, head, kv):
    z, half, width = arrived.shape
    rows = z * half
    out_shape = jax.ShapeDtypeStruct((kv, rows, 2 * LANES), jnp.bfloat16)
    scratch = [pltpu.VMEM((rows, width), jnp.float32)]
    return call(
        functools.partial(mix_kernel, head), out_shape, (arrived, own, partner), scratch, "mix"
    )


def finish_kernel(down, arrived, own, partner, residual, sent, wide):
    gathered_rows(arrived, wide)
    every = wide[...].astype(jnp.bfloat16)
    span = slice(down, down + wide.shape[1])
    side = lax.axis_index("core")
    peers, half, _ = sent.shape
    for i, weights in enumerate((own, partner)):
        total = wide_dot(every, weights[span]) + residual[i]
        to = side if i == 0 else 1 - side
        for peer in range(peers // 2):
            sent[to * (peers // 2) + peer] = total[half * peer : half * (peer + 1)]


def finish(arrived, own, partner, residual, down, kv):
    z, half, width = arrived.shape
    rows = z * half
    out_shape = jax.ShapeDtypeStruct((2 * kv, rows // kv, LANES), jnp.float32)
    scratch = [pltpu.VMEM((rows, width), jnp.float32)]
    return call(
        functools.partial(finish_kernel, down),
        out_shape,
        (arrived, own, partner, residual),
        scratch,
        "finish",
    )


def channel_kernel(
    head, units, pad, parts, stream, own_weights, partner, terms, residual, wide
):
    rows, features = stream.shape[1:]
    half = terms.shape[1]
    mixer_out = parts[0].astype(jnp.float32)
    for i in range(1, parts.shape[0]):
        mixer_out = mixer_out + parts[i].astype(jnp.float32)
    own = stream[0] + mixer_out[:, :features]
    other = stream[1] + mixer_out[:, features:]
    end = partner.shape[0]
    scaled_own, scaled_other = (
        (part * from_thirds(weights[end - GAIN_ROWS :])).astype(jnp.bfloat16)
        for part, weights in ((own, own_weights), (other, partner))
    )
    squares = jnp.sum(own * own + other * other, axis=1, keepdims=True)
    wide[:, :units] = transposed_dot(
        scaled_own, own_weights[head : head + units]
    ) + transposed_dot(
        scaled_other, partner[head : head + units]
    )
    lane = lax.broadcasted_iota(jnp.int32, (rows, pad), 1)
    wide[:, units : units + pad] = jnp.where(lane == 0, squares, 0.0)
    wide[:, units + pad :] = transposed_dot(
        scaled_own, own_weights[head + units : head + 2 * units]
    ) + transposed_dot(
        scaled_other, partner[head + units : head + 2 * units]
    )
    store_by_peer(terms, wide)
    row = lax.broadcasted_iota(jnp.int32, (rows, features), 0)
    here = row // half == lax.axis_index("kv")
    residual[0] = jnp.where(here, own, 0.0)
    residual[1] = jnp.where(here, other, 0.0)


def channel(parts, stream, own_weights, partner, head, units, z):
    pad = -units % LANES
    _, rows, features = stream.shape
    width = 2 * units + pad
    out_shape = (
        jax.ShapeDtypeStruct((z, rows // z, width), jnp.bfloat16),
        jax.ShapeDtypeStruct((2, rows, features), jnp.float32),
    )
    return call(
        functools.partial(channel_kernel, head, units, pad),
        out_shape,
        (parts, stream, own_weights, partner),
        [pltpu.VMEM((rows, width), jnp.float32)],
        "channel",
    )


def local(
    hidden_in,
    mixer_gain,
    query_weight,
    key_weight,
    value_weight,
    gate_weight,
    decay_rate,
    prior_state,
    key_block,
    value_block,
    lengths,
    group_gain,
    output_weight,
    channel_gain,
    hidden_gate,
    hidden_up,
    hidden_down,
):
    kv, z = lax.axis_size("kv"), lax.axis_size("z")
    own_rows, features = hidden_in.shape
    half = own_rows // 2
    head_width, units = output_weight.shape[0], hidden_gate.shape[1]
    weights = (
        query_weight,
        key_weight,
        value_weight,
        gate_weight,
        output_weight,
        hidden_gate.T,
        hidden_up.T,
        hidden_down,
    )
    width = sum(array.shape[1] for array in weights[:4])
    inner = width + head_width
    sent, own, table = opening(
        hidden_in, lengths, decay_rate, mixer_gain, channel_gain, weights, 2 * kv
    )
    partner = lax.ppermute(own, "core", [(0, 1), (1, 0)])
    rows = exchange(sent, ("core", "kv")).reshape(2, kv, half, features)
    terms, stream = project(rows, own, partner, width, z)
    mixed = retain(exchange(terms, "z"), table, prior_state, key_block, value_block, group_gain)
    parts = exchange(mix(exchange(mixed, "z"), own, partner, width, kv), "kv")
    terms, residual = channel(parts, stream, own, partner, inner, units, z)
    activated = activate(exchange(terms, "z"), units, -units % LANES)
    total = finish(
        exchange(activated, "z"), own, partner, residual, inner + 2 * units, kv
    )
    total = exchange(total, ("core", "kv")).reshape(2, kv, half, features)
    return jnp.sum(total, axis=1).reshape(own_rows, features).astype(jnp.bfloat16)


def solution(mesh):
    kv, tp = mesh.shape["kv"], mesh.shape["tp"]
    chips = Mesh(mesh.devices.reshape(kv, tp // 2, 2), ("kv", "z", "core"))
    tp = ("z", "core")
    in_specs = (
        P("kv", tp),
        P(tp),
        P(tp, "kv"),
        P(tp, "kv"),
        P(tp, "kv"),
        P(tp, "kv"),
        P("kv"),
        P(tp, "kv", None, None),
        P(tp, "kv", None, None),
        P(tp, "kv", None, None),
        P(tp),
        P("kv"),
        P("kv", tp),
        P(tp),
        P(tp, "kv"),
        P(tp, "kv"),
        P("kv", tp),
    )
    return jax.shard_map(
        local, mesh=chips, in_specs=in_specs, out_specs=P("kv", tp), check_vma=False
    )
```

```python
import functools

import jax
import jax.numpy as jnp
from jax import lax
from jax.experimental import pallas as pl
from jax.experimental.pallas import tpu as pltpu
from jax.sharding import Mesh
from jax.sharding import PartitionSpec as P

D = 4096
LANES = 128
BLOCK = 128


epsilon = 1e-06


def exchange(parts, axes):
    return lax.all_to_all(parts, axes, split_axis=0, concat_axis=0, tiled=True)


def from_partner(value):
    return lax.ppermute(value, "core", [(0, 1), (1, 0)])


def wide_dot(left, right):
    return jnp.dot(left, right, preferred_element_type=jnp.float32)


IN_VMEM = pl.BlockSpec(memory_space=pltpu.VMEM)
IN_HBM = pl.BlockSpec(memory_space=pltpu.HBM)
IN_SMEM = pl.BlockSpec(memory_space=pltpu.SMEM)
GAIN_ROWS = 16


def thirds(value):
    high = value.astype(jnp.bfloat16)
    rest = value - high.astype(jnp.float32)
    middle = rest.astype(jnp.bfloat16)
    return high, middle, (rest - middle.astype(jnp.float32)).astype(jnp.bfloat16)


def from_thirds(block):
    wide = block.astype(jnp.float32)
    return wide[0:1] + wide[1:2] + wide[2:3]


def store_gain(target, gain):
    high, middle, low = (part.astype(jnp.float32) for part in thirds(gain))
    row = lax.broadcasted_iota(jnp.int32, (GAIN_ROWS, LANES), 0)
    block = jnp.where(row == 0, high, jnp.where(row == 1, middle, jnp.where(row == 2, low, 0.0)))
    target[target.shape[0] - GAIN_ROWS :, :LANES] = block.astype(jnp.bfloat16)


def started(pairs, arrived):
    moves = [
        pltpu.make_async_copy(source, target, arrived.at[i])
        for i, (source, target) in enumerate(pairs)
    ]
    for move in moves:
        move.start()
    return moves


def open_kernel(hidden, gain, *refs):
    *sources, sent, joined, rows, own_gain, many, arrived = refs
    pairs, at = [(hidden, rows), (gain, own_gain)], 0
    for source in sources:
        depth, columns = source.shape
        pairs.append((source, joined.at[:depth, at : at + columns]))
        at += columns
    moves = started(pairs, arrived)
    moves[0].wait()
    peers, half, _ = many.shape
    wide = rows[...].astype(jnp.float32)
    for i in range(peers):
        first = half * (2 * i // peers)
        many[i] = wide[first : first + half].astype(jnp.bfloat16)
    out = pltpu.make_async_copy(many, sent, arrived.at[len(moves)])
    out.start()
    moves[1].wait()
    store_gain(joined, own_gain[...])
    for move in moves[2:]:
        move.wait()
    out.wait()


def held_in_hbm(*arrays):
    return [pltpu.with_memory_space_constraint(array, pltpu.HBM) for array in arrays]


def opening(hidden, gain, weights, peers):
    many = (peers, hidden.shape[0] // 2, LANES)
    joined = (LANES + GAIN_ROWS, sum(array.shape[1] for array in weights))
    operands = held_in_hbm(hidden, gain[None], *weights)
    return pl.pallas_call(
        open_kernel,
        out_shape=(
            jax.ShapeDtypeStruct(many, jnp.bfloat16),
            pltpu.VMEM(joined, jnp.bfloat16),
        ),
        in_specs=[IN_HBM] * len(operands),
        out_specs=(IN_HBM, IN_VMEM),
        scratch_shapes=[
            pltpu.VMEM(hidden.shape, jnp.bfloat16),
            pltpu.VMEM((1, LANES), jnp.float32),
            pltpu.VMEM(many, jnp.bfloat16),
            pltpu.SemaphoreType.DMA((len(operands) + 1,)),
        ],
        compiler_params=pltpu.CompilerParams(vmem_limit_bytes=8 << 20),
        cost_estimate=pl.CostEstimate(flops=2_000_000, bytes_accessed=1_000_000, transcendentals=0),
        name="opening",
    )(*operands)


def later_kernel(decay, inverse, lengths, gain, *refs):
    *sources, joined, table, place, own_gain, arrived = refs
    pairs, at = [(lengths, place), (gain, own_gain)], 0
    for source in sources:
        pairs.append((source, joined.at[at : at + source.shape[0]]))
        at += source.shape[0]
    moves = started(pairs, arrived)
    lane = lax.broadcasted_iota(jnp.int32, (1, LANES), 1)
    moves[0].wait()
    moves[1].wait()
    store_gain(joined, own_gain[...])
    seqs = place.shape[0]
    for i in range(seqs):
        angle = place[i].astype(jnp.float32) * inverse[...]
        filled = lax.rem(place[i], BLOCK)
        distance = (filled - lane).astype(jnp.float32)
        table[i : i + 1] = jnp.cos(angle)
        table[seqs + i : seqs + i + 1] = jnp.sin(angle)
        table[2 * seqs + i : 2 * seqs + i + 1] = jnp.where(
            lane < filled, jnp.exp(-decay[0] * distance), 0.0
        )
        reach = (filled + 1 + 0 * lane).astype(jnp.float32)
        table[3 * seqs + i : 3 * seqs + i + 1] = jnp.exp(-decay[0] * reach)
    for move in moves[2:]:
        move.wait()


def join_later(decay, lengths, gain, weights):
    inverse = 10000.0 ** (-jnp.arange(LANES, dtype=jnp.float32) / LANES)
    operands = held_in_hbm(lengths, gain[None], *weights)
    depth = sum(array.shape[0] for array in weights) + GAIN_ROWS
    return pl.pallas_call(
        later_kernel,
        out_shape=(
            pltpu.VMEM((depth, LANES), jnp.bfloat16),
            pltpu.VMEM((4 * lengths.shape[0], LANES), jnp.float32),
        ),
        in_specs=[IN_SMEM, IN_VMEM] + [IN_HBM] * len(operands),
        out_specs=(IN_VMEM, IN_VMEM),
        scratch_shapes=[
            pltpu.SMEM(lengths.shape, jnp.int32),
            pltpu.VMEM((1, LANES), jnp.float32),
            pltpu.SemaphoreType.DMA((len(operands),)),
        ],
        compiler_params=pltpu.CompilerParams(vmem_limit_bytes=8 << 20),
        cost_estimate=pl.CostEstimate(flops=2_000_000, bytes_accessed=1_000_000, transcendentals=0),
        name="later",
    )(decay, inverse[None], *operands)


def rotated_by(vectors, cosine, sine):
    half = cosine.shape[1]
    front, back = vectors[:, :half], vectors[:, half:]
    return jnp.concatenate([front * cosine - back * sine, front * sine + back * cosine], axis=1)


def of_each(row, products):
    result = products[0]
    for i, product in enumerate(products[1:], 1):
        result = jnp.where(row == i, product, result)
    return result


def retain_kernel(arrived, table, state, keys, values, group_gain, mixed):
    seqs, _, key_width, value_width = state.shape
    total = arrived[0].astype(jnp.float32)
    for i in range(1, arrived.shape[0]):
        total = total + arrived[i].astype(jnp.float32)
    ends = 2 * (key_width + value_width)
    scale = lax.rsqrt(total[:, ends : ends + 1] / D + epsilon)
    ready = (scale * total[:, :ends]).astype(jnp.bfloat16).astype(jnp.float32)
    cosine, sine = table[:seqs], table[seqs : 2 * seqs]
    weighting = table[2 * seqs : 3 * seqs]
    carried = table[3 * seqs :, :1]
    query = rotated_by(ready[:, :key_width], cosine, sine).astype(jnp.bfloat16)
    fresh = rotated_by(ready[:, key_width : 2 * key_width], cosine, sine) * key_width ** (-0.5)
    value = ready[:, 2 * key_width : 2 * key_width + value_width]
    gate = ready[:, 2 * key_width + value_width :]
    own = jnp.sum(query.astype(jnp.float32) * fresh, axis=1, keepdims=True) * value
    row_k = lax.broadcasted_iota(jnp.int32, (seqs, keys.shape[2]), 0)
    row_v = lax.broadcasted_iota(jnp.int32, (seqs, value_width), 0)
    scores = of_each(row_k, [transposed_dot(query, keys[i, 0]) for i in range(seqs)])
    block_weights = (scores * weighting).astype(jnp.bfloat16)
    block = of_each(row_v, [wide_dot(block_weights, values[i, 0]) for i in range(seqs)])
    remembered = []
    for i in range(seqs):
        high = state[i, 0].astype(jnp.bfloat16)
        low = (state[i, 0] - high.astype(jnp.float32)).astype(jnp.bfloat16)
        remembered.append(wide_dot(query, high) + wide_dot(query, low))
    retained = own + block + carried * of_each(row_v, remembered)
    centre = jnp.mean(retained, axis=1, keepdims=True)
    away = retained - centre
    spread = jnp.mean(away * away, axis=1, keepdims=True)
    normed = away * lax.rsqrt(spread + epsilon)
    result = (jax.nn.silu(gate) * normed * group_gain[...]).astype(jnp.bfloat16)
    for i in range(mixed.shape[0]):
        mixed[i] = result


def retain(arrived, table, state, keys, values, group_gain):
    seqs, _, _, value_width = state.shape
    out_shape = jax.ShapeDtypeStruct((arrived.shape[0], seqs, value_width), jnp.bfloat16)
    operands = (arrived, table, state, keys, values, group_gain[None])
    return call(retain_kernel, out_shape, operands, [])


def activate_kernel(units, pad, arrived, activated):
    total = arrived[0].astype(jnp.float32)
    for i in range(1, arrived.shape[0]):
        total = total + arrived[i].astype(jnp.float32)
    scale = lax.rsqrt(total[:, units : units + 1] / D + epsilon)
    gate, up = scale * total[:, :units], scale * total[:, units + pad :]
    result = (jax.nn.silu(gate) * up).astype(jnp.bfloat16)
    for i in range(activated.shape[0]):
        activated[i] = result


def activate(arrived, units, pad):
    out_shape = jax.ShapeDtypeStruct((*arrived.shape[:2], units), jnp.bfloat16)
    kernel = functools.partial(activate_kernel, units, pad)
    return call(kernel, out_shape, (arrived,), [])


def transposed_dot(left, right):
    return lax.dot_general(
        left, right, (((1,), (1,)), ((), ())), preferred_element_type=jnp.float32
    )


def store_by_peer(terms, wide):
    half = terms.shape[1]
    for i in range(terms.shape[0]):
        terms[i] = wide[half * i : half * (i + 1)].astype(jnp.bfloat16)


def gathered_rows(arrived, wide):
    half = arrived.shape[1]
    for i in range(arrived.shape[0]):
        wide[half * i : half * (i + 1)] = arrived[i].astype(jnp.float32)


def project_kernel(arrived, own, partner, terms, stream, wide):
    _, rows, features = stream.shape
    half = terms.shape[1]
    width = wide.shape[1] - LANES
    side = lax.axis_index("core")
    for i in range(rows // half):
        span = slice(half * i, half * (i + 1))
        stream[0, span] = arrived[side, i].astype(jnp.float32)
        stream[1, span] = arrived[1 - side, i].astype(jnp.float32)
    parts = [stream[i] for i in range(2)]
    total = None
    for part, weights in zip(parts, (own, partner)):
        gain = from_thirds(weights[features : features + GAIN_ROWS, :features])
        term = wide_dot((part * gain).astype(jnp.bfloat16), weights[:features])
        total = term if total is None else total + term
    wide[:, :width] = total
    squares = jnp.sum(parts[0] * parts[0] + parts[1] * parts[1], axis=1, keepdims=True)
    lane = lax.broadcasted_iota(jnp.int32, (rows, LANES), 1)
    wide[:, width:] = jnp.where(lane == 0, squares, 0.0)
    store_by_peer(terms, wide)


def call(kernel, out_shape, operands, scratch):
    return pl.pallas_call(
        kernel,
        out_shape=out_shape,
        in_specs=[IN_VMEM] * len(operands),
        out_specs=jax.tree.map(lambda _: IN_VMEM, out_shape),
        scratch_shapes=scratch,
        compiler_params=pltpu.CompilerParams(vmem_limit_bytes=8 << 20),
        cost_estimate=pl.CostEstimate(flops=8_000_000, bytes_accessed=1_000_000, transcendentals=0),
    )(*operands)


def project(arrived, own, partner, z):
    _, kv, half, features = arrived.shape
    rows = kv * half
    width = own.shape[1] + LANES
    out_shape = (
        jax.ShapeDtypeStruct((z, rows // z, width), jnp.bfloat16),
        jax.ShapeDtypeStruct((2, rows, features), jnp.float32),
    )
    scratch = [pltpu.VMEM((rows, width), jnp.float32)]
    return call(project_kernel, out_shape, (arrived, own, partner), scratch)


def mix_kernel(head, arrived, own, partner, terms, wide):
    gathered_rows(arrived, wide)
    every = wide[...].astype(jnp.bfloat16)
    span = slice(head, head + wide.shape[1])
    both = jnp.concatenate([wide_dot(every, own[span]), wide_dot(every, partner[span])], axis=1)
    both = both.astype(jnp.bfloat16)
    for i in range(terms.shape[0]):
        terms[i] = both


def mix(arrived, own, partner, head, kv):
    z, half, width = arrived.shape
    rows = z * half
    out_shape = jax.ShapeDtypeStruct((kv, rows, 2 * LANES), jnp.bfloat16)
    scratch = [pltpu.VMEM((rows, width), jnp.float32)]
    return call(functools.partial(mix_kernel, head), out_shape, (arrived, own, partner), scratch)


def finish_kernel(down, arrived, own, partner, residual, sent, wide):
    gathered_rows(arrived, wide)
    every = wide[...].astype(jnp.bfloat16)
    span = slice(down, down + wide.shape[1])
    side = lax.axis_index("core")
    peers, half, _ = sent.shape
    for i, weights in enumerate((own, partner)):
        total = wide_dot(every, weights[span]) + residual[i]
        to = side if i == 0 else 1 - side
        for peer in range(peers // 2):
            sent[to * (peers // 2) + peer] = total[half * peer : half * (peer + 1)]


def finish(arrived, own, partner, residual, down, kv):
    z, half, width = arrived.shape
    rows = z * half
    out_shape = jax.ShapeDtypeStruct((2 * kv, rows // kv, LANES), jnp.float32)
    scratch = [pltpu.VMEM((rows, width), jnp.float32)]
    return call(
        functools.partial(finish_kernel, down),
        out_shape,
        (arrived, own, partner, residual),
        scratch,
    )


def channel_kernel(
    head, units, pad, parts, stream, own_weights, partner, terms, residual, wide
):
    rows, features = stream.shape[1:]
    half = terms.shape[1]
    mixer_out = parts[0].astype(jnp.float32)
    for i in range(1, parts.shape[0]):
        mixer_out = mixer_out + parts[i].astype(jnp.float32)
    own = stream[0] + mixer_out[:, :features]
    other = stream[1] + mixer_out[:, features:]
    end = partner.shape[0]
    scaled_own, scaled_other = (
        (part * from_thirds(weights[end - GAIN_ROWS :])).astype(jnp.bfloat16)
        for part, weights in ((own, own_weights), (other, partner))
    )
    squares = jnp.sum(own * own + other * other, axis=1, keepdims=True)
    wide[:, :units] = transposed_dot(
        scaled_own, own_weights[head : head + units]
    ) + transposed_dot(
        scaled_other, partner[head : head + units]
    )
    lane = lax.broadcasted_iota(jnp.int32, (rows, pad), 1)
    wide[:, units : units + pad] = jnp.where(lane == 0, squares, 0.0)
    wide[:, units + pad :] = transposed_dot(
        scaled_own, own_weights[head + units : head + 2 * units]
    ) + transposed_dot(
        scaled_other, partner[head + units : head + 2 * units]
    )
    store_by_peer(terms, wide)
    row = lax.broadcasted_iota(jnp.int32, (rows, features), 0)
    here = row // half == lax.axis_index("kv")
    residual[0] = jnp.where(here, own, 0.0)
    residual[1] = jnp.where(here, other, 0.0)


def channel(parts, stream, own_weights, partner, head, units, z):
    pad = -units % LANES
    _, rows, features = stream.shape
    width = 2 * units + pad
    out_shape = (
        jax.ShapeDtypeStruct((z, rows // z, width), jnp.bfloat16),
        jax.ShapeDtypeStruct((2, rows, features), jnp.float32),
    )
    return call(
        functools.partial(channel_kernel, head, units, pad),
        out_shape,
        (parts, stream, own_weights, partner),
        [pltpu.VMEM((rows, width), jnp.float32)],
    )


def local(
    hidden_in,
    mixer_gain,
    query_weight,
    key_weight,
    value_weight,
    gate_weight,
    decay_rate,
    prior_state,
    key_block,
    value_block,
    lengths,
    group_gain,
    output_weight,
    channel_gain,
    hidden_gate,
    hidden_up,
    hidden_down,
):
    kv, z = lax.axis_size("kv"), lax.axis_size("z")
    own_rows, features = hidden_in.shape
    half = own_rows // 2
    head_width, units = output_weight.shape[0], hidden_gate.shape[1]
    sent, first = opening(
        hidden_in, mixer_gain, (query_weight, key_weight, value_weight, gate_weight), 2 * kv
    )
    rows = exchange(sent, ("core", "kv")).reshape(2, kv, half, features)
    first_partner = from_partner(first)
    terms, stream = project(rows, first, first_partner, z)
    arrived = exchange(terms, "z")
    later = (output_weight, hidden_gate.T, hidden_up.T, hidden_down)
    own, table = join_later(decay_rate, lengths, channel_gain, later)
    partner = from_partner(own)
    mixed = retain(arrived, table, prior_state, key_block, value_block, group_gain)
    mixed = exchange(mixed, "z")
    parts = exchange(mix(mixed, own, partner, 0, kv), "kv")
    terms, residual = channel(parts, stream, own, partner, head_width, units, z)
    activated = activate(exchange(terms, "z"), units, -units % LANES)
    total = finish(
        exchange(activated, "z"), own, partner, residual, head_width + 2 * units, kv
    )
    total = exchange(total, ("core", "kv")).reshape(2, kv, half, features)
    return jnp.sum(total, axis=1).reshape(own_rows, features).astype(jnp.bfloat16)


def solution(mesh):
    kv, tp = mesh.shape["kv"], mesh.shape["tp"]
    chips = Mesh(mesh.devices.reshape(kv, tp // 2, 2), ("kv", "z", "core"))
    tp = ("z", "core")
    in_specs = (
        P("kv", tp),
        P(tp),
        P(tp, "kv"),
        P(tp, "kv"),
        P(tp, "kv"),
        P(tp, "kv"),
        P("kv"),
        P(tp, "kv", None, None),
        P(tp, "kv", None, None),
        P(tp, "kv", None, None),
        P(tp),
        P("kv"),
        P("kv", tp),
        P(tp),
        P(tp, "kv"),
        P(tp, "kv"),
        P("kv", tp),
    )
    return jax.shard_map(
        local, mesh=chips, in_specs=in_specs, out_specs=P("kv", tp), check_vma=False
    )
```

```python
import functools

import jax
import jax.numpy as jnp
from jax import lax
from jax.experimental import pallas as pl
from jax.experimental.pallas import tpu as pltpu
from jax.sharding import Mesh
from jax.sharding import PartitionSpec as P

D = 4096
LANES = 128
BLOCK = 128
FIRST_KV = 10
FIRST_Z = 8


epsilon = 1e-06


def exchange(parts, axes, order):
    return lax.all_to_all(
        parts, axes, split_axis=0, concat_axis=0, axis_index_groups=[order], tiled=True
    )


def turned(count, first):
    return [(member + first) % count for member in range(count)]


def from_partner(value):
    return lax.ppermute(value, "core", [(0, 1), (1, 0)])


def wide_dot(left, right):
    return jnp.dot(left, right, preferred_element_type=jnp.float32)


IN_VMEM = pl.BlockSpec(memory_space=pltpu.VMEM)
IN_HBM = pl.BlockSpec(memory_space=pltpu.HBM)
IN_SMEM = pl.BlockSpec(memory_space=pltpu.SMEM)
GAIN_ROWS = 16


def thirds(value):
    high = value.astype(jnp.bfloat16)
    rest = value - high.astype(jnp.float32)
    middle = rest.astype(jnp.bfloat16)
    return high, middle, (rest - middle.astype(jnp.float32)).astype(jnp.bfloat16)


def from_thirds(block):
    wide = block.astype(jnp.float32)
    return wide[0:1] + wide[1:2] + wide[2:3]


def store_gain(target, gain):
    high, middle, low = (part.astype(jnp.float32) for part in thirds(gain))
    row = lax.broadcasted_iota(jnp.int32, (GAIN_ROWS, LANES), 0)
    block = jnp.where(row == 0, high, jnp.where(row == 1, middle, jnp.where(row == 2, low, 0.0)))
    target[target.shape[0] - GAIN_ROWS :, :LANES] = block.astype(jnp.bfloat16)


def started(pairs, arrived):
    moves = [
        pltpu.make_async_copy(source, target, arrived.at[i])
        for i, (source, target) in enumerate(pairs)
    ]
    for move in moves:
        move.start()
    return moves


def open_kernel(hidden, gain, *refs):
    *sources, sent, joined, rows, own_gain, many, arrived = refs
    pairs, at = [(hidden, rows), (gain, own_gain)], 0
    for source in sources:
        depth, columns = source.shape
        pairs.append((source, joined.at[:depth, at : at + columns]))
        at += columns
    moves = started(pairs, arrived)
    moves[0].wait()
    peers, half, _ = many.shape
    wide = rows[...].astype(jnp.float32)
    for i in range(peers):
        first = half * (2 * i // peers)
        many[i] = wide[first : first + half].astype(jnp.bfloat16)
    out = pltpu.make_async_copy(many, sent, arrived.at[len(moves)])
    out.start()
    moves[1].wait()
    store_gain(joined, own_gain[...])
    for move in moves[2:]:
        move.wait()
    out.wait()


def held_in_hbm(*arrays):
    return [pltpu.with_memory_space_constraint(array, pltpu.HBM) for array in arrays]


def opening(hidden, gain, weights, peers):
    many = (peers, hidden.shape[0] // 2, LANES)
    joined = (LANES + GAIN_ROWS, sum(array.shape[1] for array in weights))
    operands = held_in_hbm(hidden, gain[None], *weights)
    return pl.pallas_call(
        open_kernel,
        out_shape=(
            jax.ShapeDtypeStruct(many, jnp.bfloat16),
            pltpu.VMEM(joined, jnp.bfloat16),
        ),
        in_specs=[IN_HBM] * len(operands),
        out_specs=(IN_HBM, IN_VMEM),
        scratch_shapes=[
            pltpu.VMEM(hidden.shape, jnp.bfloat16),
            pltpu.VMEM((1, LANES), jnp.float32),
            pltpu.VMEM(many, jnp.bfloat16),
            pltpu.SemaphoreType.DMA((len(operands) + 1,)),
        ],
        compiler_params=pltpu.CompilerParams(vmem_limit_bytes=8 << 20),
        cost_estimate=pl.CostEstimate(flops=2_000_000, bytes_accessed=1_000_000, transcendentals=0),
        name="opening",
    )(*operands)


def later_kernel(decay, inverse, lengths, gain, *refs):
    *sources, joined, table, place, own_gain, arrived = refs
    pairs, at = [(lengths, place), (gain, own_gain)], 0
    for source in sources:
        pairs.append((source, joined.at[at : at + source.shape[0]]))
        at += source.shape[0]
    moves = started(pairs, arrived)
    lane = lax.broadcasted_iota(jnp.int32, (1, LANES), 1)
    moves[0].wait()
    moves[1].wait()
    store_gain(joined, own_gain[...])
    seqs = place.shape[0]
    for i in range(seqs):
        angle = place[i].astype(jnp.float32) * inverse[...]
        filled = lax.rem(place[i], BLOCK)
        distance = (filled - lane).astype(jnp.float32)
        table[i : i + 1] = jnp.cos(angle)
        table[seqs + i : seqs + i + 1] = jnp.sin(angle)
        table[2 * seqs + i : 2 * seqs + i + 1] = jnp.where(
            lane < filled, jnp.exp(-decay[0] * distance), 0.0
        )
        reach = (filled + 1 + 0 * lane).astype(jnp.float32)
        table[3 * seqs + i : 3 * seqs + i + 1] = jnp.exp(-decay[0] * reach)
    for move in moves[2:]:
        move.wait()


def join_later(decay, lengths, gain, weights):
    inverse = 10000.0 ** (-jnp.arange(LANES, dtype=jnp.float32) / LANES)
    operands = held_in_hbm(lengths, gain[None], *weights)
    depth = sum(array.shape[0] for array in weights) + GAIN_ROWS
    return pl.pallas_call(
        later_kernel,
        out_shape=(
            pltpu.VMEM((depth, LANES), jnp.bfloat16),
            pltpu.VMEM((4 * lengths.shape[0], LANES), jnp.float32),
        ),
        in_specs=[IN_SMEM, IN_VMEM] + [IN_HBM] * len(operands),
        out_specs=(IN_VMEM, IN_VMEM),
        scratch_shapes=[
            pltpu.SMEM(lengths.shape, jnp.int32),
            pltpu.VMEM((1, LANES), jnp.float32),
            pltpu.SemaphoreType.DMA((len(operands),)),
        ],
        compiler_params=pltpu.CompilerParams(vmem_limit_bytes=8 << 20),
        cost_estimate=pl.CostEstimate(flops=2_000_000, bytes_accessed=1_000_000, transcendentals=0),
        name="later",
    )(decay, inverse[None], *operands)


def rotated_by(vectors, cosine, sine):
    half = cosine.shape[1]
    front, back = vectors[:, :half], vectors[:, half:]
    return jnp.concatenate([front * cosine - back * sine, front * sine + back * cosine], axis=1)


def of_each(row, products):
    result = products[0]
    for i, product in enumerate(products[1:], 1):
        result = jnp.where(row == i, product, result)
    return result


def retain_kernel(arrived, table, state, keys, values, group_gain, mixed):
    seqs, _, key_width, value_width = state.shape
    total = arrived[0].astype(jnp.float32)
    for i in range(1, arrived.shape[0]):
        total = total + arrived[i].astype(jnp.float32)
    ends = 2 * (key_width + value_width)
    scale = lax.rsqrt(total[:, ends : ends + 1] / D + epsilon)
    ready = (scale * total[:, :ends]).astype(jnp.bfloat16).astype(jnp.float32)
    cosine, sine = table[:seqs], table[seqs : 2 * seqs]
    weighting = table[2 * seqs : 3 * seqs]
    carried = table[3 * seqs :, :1]
    query = rotated_by(ready[:, :key_width], cosine, sine).astype(jnp.bfloat16)
    fresh = rotated_by(ready[:, key_width : 2 * key_width], cosine, sine) * key_width ** (-0.5)
    value = ready[:, 2 * key_width : 2 * key_width + value_width]
    gate = ready[:, 2 * key_width + value_width :]
    own = jnp.sum(query.astype(jnp.float32) * fresh, axis=1, keepdims=True) * value
    row_k = lax.broadcasted_iota(jnp.int32, (seqs, keys.shape[2]), 0)
    row_v = lax.broadcasted_iota(jnp.int32, (seqs, value_width), 0)
    scores = of_each(row_k, [transposed_dot(query, keys[i, 0]) for i in range(seqs)])
    block_weights = (scores * weighting).astype(jnp.bfloat16)
    block = of_each(row_v, [wide_dot(block_weights, values[i, 0]) for i in range(seqs)])
    remembered = []
    for i in range(seqs):
        high = state[i, 0].astype(jnp.bfloat16)
        low = (state[i, 0] - high.astype(jnp.float32)).astype(jnp.bfloat16)
        remembered.append(wide_dot(query, high) + wide_dot(query, low))
    retained = own + block + carried * of_each(row_v, remembered)
    centre = jnp.mean(retained, axis=1, keepdims=True)
    away = retained - centre
    spread = jnp.mean(away * away, axis=1, keepdims=True)
    normed = away * lax.rsqrt(spread + epsilon)
    result = (jax.nn.silu(gate) * normed * group_gain[...]).astype(jnp.bfloat16)
    for i in range(mixed.shape[0]):
        mixed[i] = result


def retain(arrived, table, state, keys, values, group_gain):
    seqs, _, _, value_width = state.shape
    out_shape = jax.ShapeDtypeStruct((arrived.shape[0], seqs, value_width), jnp.bfloat16)
    operands = (arrived, table, state, keys, values, group_gain[None])
    return call(retain_kernel, out_shape, operands, [])


def activate_kernel(units, pad, arrived, activated):
    total = arrived[0].astype(jnp.float32)
    for i in range(1, arrived.shape[0]):
        total = total + arrived[i].astype(jnp.float32)
    scale = lax.rsqrt(total[:, units : units + 1] / D + epsilon)
    gate, up = scale * total[:, :units], scale * total[:, units + pad :]
    result = (jax.nn.silu(gate) * up).astype(jnp.bfloat16)
    for i in range(activated.shape[0]):
        activated[i] = result


def activate(arrived, units, pad):
    out_shape = jax.ShapeDtypeStruct((*arrived.shape[:2], units), jnp.bfloat16)
    kernel = functools.partial(activate_kernel, units, pad)
    return call(kernel, out_shape, (arrived,), [])


def transposed_dot(left, right):
    return lax.dot_general(
        left, right, (((1,), (1,)), ((), ())), preferred_element_type=jnp.float32
    )


def store_by_peer(terms, wide):
    half = terms.shape[1]
    for i in range(terms.shape[0]):
        terms[i] = wide[half * i : half * (i + 1)].astype(jnp.bfloat16)


def gathered_rows(arrived, wide):
    half = arrived.shape[1]
    for i in range(arrived.shape[0]):
        wide[half * i : half * (i + 1)] = arrived[i].astype(jnp.float32)


def project_kernel(arrived, own, partner, terms, stream, wide):
    _, rows, features = stream.shape
    half = terms.shape[1]
    width = wide.shape[1] - LANES
    side = lax.axis_index("core")
    for i in range(rows // half):
        span = slice(half * i, half * (i + 1))
        source = (i + FIRST_Z - FIRST_KV) % (rows // half)
        stream[0, span] = arrived[side, source].astype(jnp.float32)
        stream[1, span] = arrived[1 - side, source].astype(jnp.float32)
    parts = [stream[i] for i in range(2)]
    total = None
    for part, weights in zip(parts, (own, partner)):
        gain = from_thirds(weights[features : features + GAIN_ROWS, :features])
        term = wide_dot((part * gain).astype(jnp.bfloat16), weights[:features])
        total = term if total is None else total + term
    wide[:, :width] = total
    squares = jnp.sum(parts[0] * parts[0] + parts[1] * parts[1], axis=1, keepdims=True)
    lane = lax.broadcasted_iota(jnp.int32, (rows, LANES), 1)
    wide[:, width:] = jnp.where(lane == 0, squares, 0.0)
    store_by_peer(terms, wide)


def call(kernel, out_shape, operands, scratch):
    return pl.pallas_call(
        kernel,
        out_shape=out_shape,
        in_specs=[IN_VMEM] * len(operands),
        out_specs=jax.tree.map(lambda _: IN_VMEM, out_shape),
        scratch_shapes=scratch,
        compiler_params=pltpu.CompilerParams(vmem_limit_bytes=8 << 20),
        cost_estimate=pl.CostEstimate(flops=8_000_000, bytes_accessed=1_000_000, transcendentals=0),
    )(*operands)


def project(arrived, own, partner, z):
    _, kv, half, features = arrived.shape
    rows = kv * half
    width = own.shape[1] + LANES
    out_shape = (
        jax.ShapeDtypeStruct((z, rows // z, width), jnp.bfloat16),
        jax.ShapeDtypeStruct((2, rows, features), jnp.float32),
    )
    scratch = [pltpu.VMEM((rows, width), jnp.float32)]
    return call(project_kernel, out_shape, (arrived, own, partner), scratch)


def mix_kernel(head, arrived, own, partner, terms, wide):
    gathered_rows(arrived, wide)
    every = wide[...].astype(jnp.bfloat16)
    span = slice(head, head + wide.shape[1])
    both = jnp.concatenate([wide_dot(every, own[span]), wide_dot(every, partner[span])], axis=1)
    both = both.astype(jnp.bfloat16)
    for i in range(terms.shape[0]):
        terms[i] = both


def mix(arrived, own, partner, head, kv):
    z, half, width = arrived.shape
    rows = z * half
    out_shape = jax.ShapeDtypeStruct((kv, rows, 2 * LANES), jnp.bfloat16)
    scratch = [pltpu.VMEM((rows, width), jnp.float32)]
    return call(functools.partial(mix_kernel, head), out_shape, (arrived, own, partner), scratch)


def finish_kernel(down, arrived, own, partner, residual, sent, wide):
    gathered_rows(arrived, wide)
    every = wide[...].astype(jnp.bfloat16)
    span = slice(down, down + wide.shape[1])
    side = lax.axis_index("core")
    peers, half, _ = sent.shape
    for i, weights in enumerate((own, partner)):
        total = wide_dot(every, weights[span]) + residual[i]
        to = side if i == 0 else 1 - side
        for peer in range(peers // 2):
            at = half * ((peer + FIRST_KV - FIRST_Z) % (peers // 2))
            sent[to * (peers // 2) + peer] = total[at : at + half]


def finish(arrived, own, partner, residual, down, kv):
    z, half, width = arrived.shape
    rows = z * half
    out_shape = jax.ShapeDtypeStruct((2 * kv, rows // kv, LANES), jnp.float32)
    scratch = [pltpu.VMEM((rows, width), jnp.float32)]
    return call(
        functools.partial(finish_kernel, down),
        out_shape,
        (arrived, own, partner, residual),
        scratch,
    )


def channel_kernel(
    head, units, pad, parts, stream, own_weights, partner, terms, residual, wide
):
    rows, features = stream.shape[1:]
    half = terms.shape[1]
    mixer_out = parts[0].astype(jnp.float32)
    for i in range(1, parts.shape[0]):
        mixer_out = mixer_out + parts[i].astype(jnp.float32)
    own = stream[0] + mixer_out[:, :features]
    other = stream[1] + mixer_out[:, features:]
    end = partner.shape[0]
    scaled_own, scaled_other = (
        (part * from_thirds(weights[end - GAIN_ROWS :])).astype(jnp.bfloat16)
        for part, weights in ((own, own_weights), (other, partner))
    )
    squares = jnp.sum(own * own + other * other, axis=1, keepdims=True)
    wide[:, :units] = transposed_dot(
        scaled_own, own_weights[head : head + units]
    ) + transposed_dot(
        scaled_other, partner[head : head + units]
    )
    lane = lax.broadcasted_iota(jnp.int32, (rows, pad), 1)
    wide[:, units : units + pad] = jnp.where(lane == 0, squares, 0.0)
    wide[:, units + pad :] = transposed_dot(
        scaled_own, own_weights[head + units : head + 2 * units]
    ) + transposed_dot(
        scaled_other, partner[head + units : head + 2 * units]
    )
    store_by_peer(terms, wide)
    row = lax.broadcasted_iota(jnp.int32, (rows, features), 0)
    peers = rows // half
    here = lax.rem(row // half + FIRST_Z, peers) == lax.axis_index("kv")
    residual[0] = jnp.where(here, own, 0.0)
    residual[1] = jnp.where(here, other, 0.0)


def channel(parts, stream, own_weights, partner, head, units, z):
    pad = -units % LANES
    _, rows, features = stream.shape
    width = 2 * units + pad
    out_shape = (
        jax.ShapeDtypeStruct((z, rows // z, width), jnp.bfloat16),
        jax.ShapeDtypeStruct((2, rows, features), jnp.float32),
    )
    return call(
        functools.partial(channel_kernel, head, units, pad),
        out_shape,
        (parts, stream, own_weights, partner),
        [pltpu.VMEM((rows, width), jnp.float32)],
    )


def local(
    hidden_in,
    mixer_gain,
    query_weight,
    key_weight,
    value_weight,
    gate_weight,
    decay_rate,
    prior_state,
    key_block,
    value_block,
    lengths,
    group_gain,
    output_weight,
    channel_gain,
    hidden_gate,
    hidden_up,
    hidden_down,
):
    kv, z = lax.axis_size("kv"), lax.axis_size("z")
    own_rows, features = hidden_in.shape
    half = own_rows // 2
    head_width, units = output_weight.shape[0], hidden_gate.shape[1]
    line = turned(z, FIRST_Z)
    plane = [side * kv + member for side in range(2) for member in turned(kv, FIRST_KV)]
    sent, first = opening(
        hidden_in, mixer_gain, (query_weight, key_weight, value_weight, gate_weight), 2 * kv
    )
    rows = exchange(sent, ("core", "kv"), plane).reshape(2, kv, half, features)
    first_partner = from_partner(first)
    terms, stream = project(rows, first, first_partner, z)
    arrived = exchange(terms, "z", line)
    later = (output_weight, hidden_gate.T, hidden_up.T, hidden_down)
    own, table = join_later(decay_rate, lengths, channel_gain, later)
    partner = from_partner(own)
    mixed = retain(arrived, table, prior_state, key_block, value_block, group_gain)
    mixed = exchange(mixed, "z", line)
    parts = exchange(mix(mixed, own, partner, 0, kv), "kv", turned(kv, FIRST_KV))
    terms, residual = channel(parts, stream, own, partner, head_width, units, z)
    activated = activate(exchange(terms, "z", line), units, -units % LANES)
    total = finish(
        exchange(activated, "z", line), own, partner, residual, head_width + 2 * units, kv
    )
    total = exchange(total, ("core", "kv"), plane).reshape(2, kv, half, features)
    return jnp.sum(total, axis=1).reshape(own_rows, features).astype(jnp.bfloat16)


def solution(mesh):
    kv, tp = mesh.shape["kv"], mesh.shape["tp"]
    chips = Mesh(mesh.devices.reshape(kv, tp // 2, 2), ("kv", "z", "core"))
    tp = ("z", "core")
    in_specs = (
        P("kv", tp),
        P(tp),
        P(tp, "kv"),
        P(tp, "kv"),
        P(tp, "kv"),
        P(tp, "kv"),
        P("kv"),
        P(tp, "kv", None, None),
        P(tp, "kv", None, None),
        P(tp, "kv", None, None),
        P(tp),
        P("kv"),
        P("kv", tp),
        P(tp),
        P(tp, "kv"),
        P(tp, "kv"),
        P("kv", tp),
    )
    return jax.shard_map(
        local, mesh=chips, in_specs=in_specs, out_specs=P("kv", tp), check_vma=False
    )
```

```python
import functools

import jax
import jax.numpy as jnp
from jax import lax
from jax.experimental import pallas as pl
from jax.experimental.pallas import tpu as pltpu
from jax.sharding import Mesh
from jax.sharding import PartitionSpec as P

D = 4096
LANES = 128
BLOCK = 128
SPREAD_AT, SUM_AT, RETURN_AT = 10, 10, 10
HEADS_AT, MIXED_AT, UNITS_AT, ACTIVE_AT = 9, 9, 9, 9
SPREAD_SIDES, RETURN_SIDES = (1, 0), (0, 1)


epsilon = 1e-06


def exchange(parts, axes, order):
    return lax.all_to_all(
        parts, axes, split_axis=0, concat_axis=0, axis_index_groups=[order], tiled=True
    )


def turned(count, first):
    return [(member + first) % count for member in range(count)]


def from_partner(value):
    return lax.ppermute(value, "core", [(0, 1), (1, 0)])


def wide_dot(left, right):
    return jnp.dot(left, right, preferred_element_type=jnp.float32)


IN_VMEM = pl.BlockSpec(memory_space=pltpu.VMEM)
IN_HBM = pl.BlockSpec(memory_space=pltpu.HBM)
IN_SMEM = pl.BlockSpec(memory_space=pltpu.SMEM)
GAIN_ROWS = 16


def thirds(value):
    high = value.astype(jnp.bfloat16)
    rest = value - high.astype(jnp.float32)
    middle = rest.astype(jnp.bfloat16)
    return high, middle, (rest - middle.astype(jnp.float32)).astype(jnp.bfloat16)


def from_thirds(block):
    wide = block.astype(jnp.float32)
    return wide[0:1] + wide[1:2] + wide[2:3]


def store_gain(target, gain):
    high, middle, low = (part.astype(jnp.float32) for part in thirds(gain))
    row = lax.broadcasted_iota(jnp.int32, (GAIN_ROWS, LANES), 0)
    block = jnp.where(row == 0, high, jnp.where(row == 1, middle, jnp.where(row == 2, low, 0.0)))
    target[target.shape[0] - GAIN_ROWS :, :LANES] = block.astype(jnp.bfloat16)


def started(pairs, arrived):
    moves = [
        pltpu.make_async_copy(source, target, arrived.at[i])
        for i, (source, target) in enumerate(pairs)
    ]
    for move in moves:
        move.start()
    return moves


def open_kernel(hidden, gain, *refs):
    *sources, sent, joined, rows, own_gain, many, arrived = refs
    pairs, at = [(hidden, rows), (gain, own_gain)], 0
    for source in sources:
        depth, columns = source.shape
        pairs.append((source, joined.at[:depth, at : at + columns]))
        at += columns
    moves = started(pairs, arrived)
    moves[0].wait()
    peers, half, _ = many.shape
    wide = rows[...].astype(jnp.float32)
    for i in range(peers):
        first = half * SPREAD_SIDES[2 * i // peers]
        many[i] = wide[first : first + half].astype(jnp.bfloat16)
    out = pltpu.make_async_copy(many, sent, arrived.at[len(moves)])
    out.start()
    moves[1].wait()
    store_gain(joined, own_gain[...])
    for move in moves[2:]:
        move.wait()
    out.wait()


def held_in_hbm(*arrays):
    return [pltpu.with_memory_space_constraint(array, pltpu.HBM) for array in arrays]


def opening(hidden, gain, weights, peers):
    many = (peers, hidden.shape[0] // 2, LANES)
    joined = (LANES + GAIN_ROWS, sum(array.shape[1] for array in weights))
    operands = held_in_hbm(hidden, gain[None], *weights)
    return pl.pallas_call(
        open_kernel,
        out_shape=(
            jax.ShapeDtypeStruct(many, jnp.bfloat16),
            pltpu.VMEM(joined, jnp.bfloat16),
        ),
        in_specs=[IN_HBM] * len(operands),
        out_specs=(IN_HBM, IN_VMEM),
        scratch_shapes=[
            pltpu.VMEM(hidden.shape, jnp.bfloat16),
            pltpu.VMEM((1, LANES), jnp.float32),
            pltpu.VMEM(many, jnp.bfloat16),
            pltpu.SemaphoreType.DMA((len(operands) + 1,)),
        ],
        compiler_params=pltpu.CompilerParams(vmem_limit_bytes=8 << 20),
        cost_estimate=pl.CostEstimate(flops=2_000_000, bytes_accessed=1_000_000, transcendentals=0),
        name="opening",
    )(*operands)


def later_kernel(decay, inverse, lengths, gain, *refs):
    *sources, joined, table, place, own_gain, arrived = refs
    pairs, at = [(lengths, place), (gain, own_gain)], 0
    for source in sources:
        pairs.append((source, joined.at[at : at + source.shape[0]]))
        at += source.shape[0]
    moves = started(pairs, arrived)
    lane = lax.broadcasted_iota(jnp.int32, (1, LANES), 1)
    moves[0].wait()
    moves[1].wait()
    store_gain(joined, own_gain[...])
    seqs = place.shape[0]
    for i in range(seqs):
        angle = place[i].astype(jnp.float32) * inverse[...]
        filled = lax.rem(place[i], BLOCK)
        distance = (filled - lane).astype(jnp.float32)
        table[i : i + 1] = jnp.cos(angle)
        table[seqs + i : seqs + i + 1] = jnp.sin(angle)
        table[2 * seqs + i : 2 * seqs + i + 1] = jnp.where(
            lane < filled, jnp.exp(-decay[0] * distance), 0.0
        )
        reach = (filled + 1 + 0 * lane).astype(jnp.float32)
        table[3 * seqs + i : 3 * seqs + i + 1] = jnp.exp(-decay[0] * reach)
    for move in moves[2:]:
        move.wait()


def join_later(decay, lengths, gain, weights):
    inverse = 10000.0 ** (-jnp.arange(LANES, dtype=jnp.float32) / LANES)
    operands = held_in_hbm(lengths, gain[None], *weights)
    depth = sum(array.shape[0] for array in weights) + GAIN_ROWS
    return pl.pallas_call(
        later_kernel,
        out_shape=(
            pltpu.VMEM((depth, LANES), jnp.bfloat16),
            pltpu.VMEM((4 * lengths.shape[0], LANES), jnp.float32),
        ),
        in_specs=[IN_SMEM, IN_VMEM] + [IN_HBM] * len(operands),
        out_specs=(IN_VMEM, IN_VMEM),
        scratch_shapes=[
            pltpu.SMEM(lengths.shape, jnp.int32),
            pltpu.VMEM((1, LANES), jnp.float32),
            pltpu.SemaphoreType.DMA((len(operands),)),
        ],
        compiler_params=pltpu.CompilerParams(vmem_limit_bytes=8 << 20),
        cost_estimate=pl.CostEstimate(flops=2_000_000, bytes_accessed=1_000_000, transcendentals=0),
        name="later",
    )(decay, inverse[None], *operands)


def rotated_by(vectors, cosine, sine):
    half = cosine.shape[1]
    front, back = vectors[:, :half], vectors[:, half:]
    return jnp.concatenate([front * cosine - back * sine, front * sine + back * cosine], axis=1)


def of_each(row, products):
    result = products[0]
    for i, product in enumerate(products[1:], 1):
        result = jnp.where(row == i, product, result)
    return result


def retain_kernel(arrived, table, state, keys, values, group_gain, mixed):
    seqs, _, key_width, value_width = state.shape
    total = arrived[0].astype(jnp.float32)
    for i in range(1, arrived.shape[0]):
        total = total + arrived[i].astype(jnp.float32)
    ends = 2 * (key_width + value_width)
    scale = lax.rsqrt(total[:, ends : ends + 1] / D + epsilon)
    ready = (scale * total[:, :ends]).astype(jnp.bfloat16).astype(jnp.float32)
    cosine, sine = table[:seqs], table[seqs : 2 * seqs]
    weighting = table[2 * seqs : 3 * seqs]
    carried = table[3 * seqs :, :1]
    query = rotated_by(ready[:, :key_width], cosine, sine).astype(jnp.bfloat16)
    fresh = rotated_by(ready[:, key_width : 2 * key_width], cosine, sine) * key_width ** (-0.5)
    value = ready[:, 2 * key_width : 2 * key_width + value_width]
    gate = ready[:, 2 * key_width + value_width :]
    own = jnp.sum(query.astype(jnp.float32) * fresh, axis=1, keepdims=True) * value
    row_k = lax.broadcasted_iota(jnp.int32, (seqs, keys.shape[2]), 0)
    row_v = lax.broadcasted_iota(jnp.int32, (seqs, value_width), 0)
    scores = of_each(row_k, [transposed_dot(query, keys[i, 0]) for i in range(seqs)])
    block_weights = (scores * weighting).astype(jnp.bfloat16)
    block = of_each(row_v, [wide_dot(block_weights, values[i, 0]) for i in range(seqs)])
    remembered = []
    for i in range(seqs):
        high = state[i, 0].astype(jnp.bfloat16)
        low = (state[i, 0] - high.astype(jnp.float32)).astype(jnp.bfloat16)
        remembered.append(wide_dot(query, high) + wide_dot(query, low))
    retained = own + block + carried * of_each(row_v, remembered)
    centre = jnp.mean(retained, axis=1, keepdims=True)
    away = retained - centre
    spread = jnp.mean(away * away, axis=1, keepdims=True)
    normed = away * lax.rsqrt(spread + epsilon)
    result = (jax.nn.silu(gate) * normed * group_gain[...]).astype(jnp.bfloat16)
    for i in range(mixed.shape[0]):
        mixed[i] = result


def retain(arrived, table, state, keys, values, group_gain):
    seqs, _, _, value_width = state.shape
    out_shape = jax.ShapeDtypeStruct((arrived.shape[0], seqs, value_width), jnp.bfloat16)
    operands = (arrived, table, state, keys, values, group_gain[None])
    return call(retain_kernel, out_shape, operands, [])


def activate_kernel(units, pad, arrived, activated):
    total = arrived[0].astype(jnp.float32)
    for i in range(1, arrived.shape[0]):
        total = total + arrived[i].astype(jnp.float32)
    scale = lax.rsqrt(total[:, units : units + 1] / D + epsilon)
    gate, up = scale * total[:, :units], scale * total[:, units + pad :]
    result = (jax.nn.silu(gate) * up).astype(jnp.bfloat16)
    for i in range(activated.shape[0]):
        activated[i] = result


def activate(arrived, units, pad):
    out_shape = jax.ShapeDtypeStruct((*arrived.shape[:2], units), jnp.bfloat16)
    kernel = functools.partial(activate_kernel, units, pad)
    return call(kernel, out_shape, (arrived,), [])


def transposed_dot(left, right):
    return lax.dot_general(
        left, right, (((1,), (1,)), ((), ())), preferred_element_type=jnp.float32
    )


def store_by_peer(terms, wide, first):
    peers, half, _ = terms.shape
    for i in range(peers):
        at = half * ((i + first) % peers)
        terms[i] = wide[at : at + half].astype(jnp.bfloat16)


def gathered_rows(arrived, wide, first):
    peers, half, _ = arrived.shape
    for i in range(peers):
        at = half * ((i + first) % peers)
        wide[at : at + half] = arrived[i].astype(jnp.float32)


def project_kernel(arrived, own, partner, terms, stream, wide):
    _, rows, features = stream.shape
    half = terms.shape[1]
    width = wide.shape[1] - LANES
    side = lax.axis_index("core")
    place = side if SPREAD_SIDES[0] == 0 else 1 - side
    for i in range(rows // half):
        span = slice(half * i, half * (i + 1))
        source = (i - SPREAD_AT) % (rows // half)
        stream[0, span] = arrived[place, source].astype(jnp.float32)
        stream[1, span] = arrived[1 - place, source].astype(jnp.float32)
    parts = [stream[i] for i in range(2)]
    total = None
    for part, weights in zip(parts, (own, partner)):
        gain = from_thirds(weights[features : features + GAIN_ROWS, :features])
        term = wide_dot((part * gain).astype(jnp.bfloat16), weights[:features])
        total = term if total is None else total + term
    wide[:, :width] = total
    squares = jnp.sum(parts[0] * parts[0] + parts[1] * parts[1], axis=1, keepdims=True)
    lane = lax.broadcasted_iota(jnp.int32, (rows, LANES), 1)
    wide[:, width:] = jnp.where(lane == 0, squares, 0.0)
    store_by_peer(terms, wide, HEADS_AT)


def call(kernel, out_shape, operands, scratch):
    return pl.pallas_call(
        kernel,
        out_shape=out_shape,
        in_specs=[IN_VMEM] * len(operands),
        out_specs=jax.tree.map(lambda _: IN_VMEM, out_shape),
        scratch_shapes=scratch,
        compiler_params=pltpu.CompilerParams(vmem_limit_bytes=8 << 20),
        cost_estimate=pl.CostEstimate(flops=8_000_000, bytes_accessed=1_000_000, transcendentals=0),
    )(*operands)


def project(arrived, own, partner, z):
    _, kv, half, features = arrived.shape
    rows = kv * half
    width = own.shape[1] + LANES
    out_shape = (
        jax.ShapeDtypeStruct((z, rows // z, width), jnp.bfloat16),
        jax.ShapeDtypeStruct((2, rows, features), jnp.float32),
    )
    scratch = [pltpu.VMEM((rows, width), jnp.float32)]
    return call(project_kernel, out_shape, (arrived, own, partner), scratch)


def mix_kernel(head, arrived, own, partner, terms, wide):
    gathered_rows(arrived, wide, MIXED_AT)
    every = wide[...].astype(jnp.bfloat16)
    span = slice(head, head + wide.shape[1])
    both = jnp.concatenate([wide_dot(every, own[span]), wide_dot(every, partner[span])], axis=1)
    both = both.astype(jnp.bfloat16)
    for i in range(terms.shape[0]):
        terms[i] = both


def mix(arrived, own, partner, head, kv):
    z, half, width = arrived.shape
    rows = z * half
    out_shape = jax.ShapeDtypeStruct((kv, rows, 2 * LANES), jnp.bfloat16)
    scratch = [pltpu.VMEM((rows, width), jnp.float32)]
    return call(functools.partial(mix_kernel, head), out_shape, (arrived, own, partner), scratch)


def finish_kernel(down, arrived, own, partner, residual, sent, wide):
    gathered_rows(arrived, wide, ACTIVE_AT)
    every = wide[...].astype(jnp.bfloat16)
    span = slice(down, down + wide.shape[1])
    side = lax.axis_index("core")
    place = side if RETURN_SIDES[0] == 0 else 1 - side
    peers, half, _ = sent.shape
    for i, weights in enumerate((own, partner)):
        total = wide_dot(every, weights[span]) + residual[i]
        to = place if i == 0 else 1 - place
        for peer in range(peers // 2):
            at = half * ((peer + RETURN_AT) % (peers // 2))
            sent[to * (peers // 2) + peer] = total[at : at + half]


def finish(arrived, own, partner, residual, down, kv):
    z, half, width = arrived.shape
    rows = z * half
    out_shape = jax.ShapeDtypeStruct((2 * kv, rows // kv, LANES), jnp.float32)
    scratch = [pltpu.VMEM((rows, width), jnp.float32)]
    return call(
        functools.partial(finish_kernel, down),
        out_shape,
        (arrived, own, partner, residual),
        scratch,
    )


def channel_kernel(
    head, units, pad, parts, stream, own_weights, partner, terms, residual, wide
):
    rows, features = stream.shape[1:]
    half = terms.shape[1]
    mixer_out = parts[0].astype(jnp.float32)
    for i in range(1, parts.shape[0]):
        mixer_out = mixer_out + parts[i].astype(jnp.float32)
    own = stream[0] + mixer_out[:, :features]
    other = stream[1] + mixer_out[:, features:]
    end = partner.shape[0]
    scaled_own, scaled_other = (
        (part * from_thirds(weights[end - GAIN_ROWS :])).astype(jnp.bfloat16)
        for part, weights in ((own, own_weights), (other, partner))
    )
    squares = jnp.sum(own * own + other * other, axis=1, keepdims=True)
    wide[:, :units] = transposed_dot(
        scaled_own, own_weights[head : head + units]
    ) + transposed_dot(
        scaled_other, partner[head : head + units]
    )
    lane = lax.broadcasted_iota(jnp.int32, (rows, pad), 1)
    wide[:, units : units + pad] = jnp.where(lane == 0, squares, 0.0)
    wide[:, units + pad :] = transposed_dot(
        scaled_own, own_weights[head + units : head + 2 * units]
    ) + transposed_dot(
        scaled_other, partner[head + units : head + 2 * units]
    )
    store_by_peer(terms, wide, UNITS_AT)
    row = lax.broadcasted_iota(jnp.int32, (rows, features), 0)
    here = row // half == lax.axis_index("kv")
    residual[0] = jnp.where(here, own, 0.0)
    residual[1] = jnp.where(here, other, 0.0)


def channel(parts, stream, own_weights, partner, head, units, z):
    pad = -units % LANES
    _, rows, features = stream.shape
    width = 2 * units + pad
    out_shape = (
        jax.ShapeDtypeStruct((z, rows // z, width), jnp.bfloat16),
        jax.ShapeDtypeStruct((2, rows, features), jnp.float32),
    )
    return call(
        functools.partial(channel_kernel, head, units, pad),
        out_shape,
        (parts, stream, own_weights, partner),
        [pltpu.VMEM((rows, width), jnp.float32)],
    )


def local(
    hidden_in,
    mixer_gain,
    query_weight,
    key_weight,
    value_weight,
    gate_weight,
    decay_rate,
    prior_state,
    key_block,
    value_block,
    lengths,
    group_gain,
    output_weight,
    channel_gain,
    hidden_gate,
    hidden_up,
    hidden_down,
):
    kv, z = lax.axis_size("kv"), lax.axis_size("z")
    own_rows, features = hidden_in.shape
    half = own_rows // 2
    head_width, units = output_weight.shape[0], hidden_gate.shape[1]
    spread, back = (
        [side * kv + member for side in sides for member in turned(kv, first)]
        for sides, first in ((SPREAD_SIDES, SPREAD_AT), (RETURN_SIDES, RETURN_AT))
    )
    sent, first = opening(
        hidden_in, mixer_gain, (query_weight, key_weight, value_weight, gate_weight), 2 * kv
    )
    rows = exchange(sent, ("core", "kv"), spread).reshape(2, kv, half, features)
    first_partner = from_partner(first)
    terms, stream = project(rows, first, first_partner, z)
    arrived = exchange(terms, "z", turned(z, HEADS_AT))
    later = (output_weight, hidden_gate.T, hidden_up.T, hidden_down)
    own, table = join_later(decay_rate, lengths, channel_gain, later)
    partner = from_partner(own)
    mixed = retain(arrived, table, prior_state, key_block, value_block, group_gain)
    mixed = exchange(mixed, "z", turned(z, MIXED_AT))
    parts = exchange(mix(mixed, own, partner, 0, kv), "kv", turned(kv, SUM_AT))
    terms, residual = channel(parts, stream, own, partner, head_width, units, z)
    activated = activate(exchange(terms, "z", turned(z, UNITS_AT)), units, -units % LANES)
    total = finish(
        exchange(activated, "z", turned(z, ACTIVE_AT)), own, partner, residual, head_width + 2 * units, kv
    )
    total = exchange(total, ("core", "kv"), back).reshape(2, kv, half, features)
    total = total if RETURN_SIDES[0] == 0 else total[::-1]
    return jnp.sum(total, axis=1).reshape(own_rows, features).astype(jnp.bfloat16)


def solution(mesh):
    kv, tp = mesh.shape["kv"], mesh.shape["tp"]
    chips = Mesh(mesh.devices.reshape(kv, tp // 2, 2), ("kv", "z", "core"))
    tp = ("z", "core")
    in_specs = (
        P("kv", tp),
        P(tp),
        P(tp, "kv"),
        P(tp, "kv"),
        P(tp, "kv"),
        P(tp, "kv"),
        P("kv"),
        P(tp, "kv", None, None),
        P(tp, "kv", None, None),
        P(tp, "kv", None, None),
        P(tp),
        P("kv"),
        P("kv", tp),
        P(tp),
        P(tp, "kv"),
        P(tp, "kv"),
        P("kv", tp),
    )
    return jax.shard_map(
        local, mesh=chips, in_specs=in_specs, out_specs=P("kv", tp), check_vma=False
    )
```

```python
import functools

import jax
import jax.numpy as jnp
from jax import lax
from jax.experimental import pallas as pl
from jax.experimental.pallas import tpu as pltpu
from jax.sharding import Mesh
from jax.sharding import PartitionSpec as P

D = 4096
LANES = 128
BLOCK = 128
SPREAD_AT, SUM_AT, RETURN_AT = 10, 10, 10
HEADS_AT, MIXED_AT, UNITS_AT, ACTIVE_AT = 9, 9, 9, 9
SPREAD_SIDES, RETURN_SIDES = (1, 0), (0, 1)


epsilon = 1e-06


def exchange(parts, axes, order):
    return lax.all_to_all(
        parts, axes, split_axis=0, concat_axis=0, axis_index_groups=[order], tiled=True
    )


def turned(count, first):
    return [(member + first) % count for member in range(count)]


def from_partner(value):
    return lax.ppermute(value, "core", [(0, 1), (1, 0)])


def wide_dot(left, right):
    return jnp.dot(left, right, preferred_element_type=jnp.float32)


IN_VMEM = pl.BlockSpec(memory_space=pltpu.VMEM)
IN_HBM = pl.BlockSpec(memory_space=pltpu.HBM)
IN_SMEM = pl.BlockSpec(memory_space=pltpu.SMEM)
GAIN_ROWS = 16


def thirds(value):
    high = value.astype(jnp.bfloat16)
    rest = value - high.astype(jnp.float32)
    middle = rest.astype(jnp.bfloat16)
    return high, middle, (rest - middle.astype(jnp.float32)).astype(jnp.bfloat16)


def from_thirds(block):
    wide = block.astype(jnp.float32)
    return wide[0:1] + wide[1:2] + wide[2:3]


def store_gain(target, gain):
    high, middle, low = (part.astype(jnp.float32) for part in thirds(gain))
    row = lax.broadcasted_iota(jnp.int32, (GAIN_ROWS, LANES), 0)
    block = jnp.where(row == 0, high, jnp.where(row == 1, middle, jnp.where(row == 2, low, 0.0)))
    target[target.shape[0] - GAIN_ROWS :, :LANES] = block.astype(jnp.bfloat16)


def started(pairs, arrived):
    moves = [
        pltpu.make_async_copy(source, target, arrived.at[i])
        for i, (source, target) in enumerate(pairs)
    ]
    for move in moves:
        move.start()
    return moves


def open_kernel(hidden, gain, *refs):
    *sources, sent, joined, rows, own_gain, many, arrived = refs
    pairs, at = [(hidden, rows), (gain, own_gain)], 0
    for source in sources:
        depth, columns = source.shape
        for lane in range(0, columns, LANES):
            pairs.append((source.at[:, lane : lane + LANES], joined.at[at : at + depth]))
            at += depth
    moves = started(pairs, arrived)
    moves[0].wait()
    peers, half, _ = many.shape
    wide = rows[...].astype(jnp.float32)
    for i in range(peers):
        first = half * SPREAD_SIDES[2 * i // peers]
        many[i] = wide[first : first + half].astype(jnp.bfloat16)
    out = pltpu.make_async_copy(many, sent, arrived.at[len(moves)])
    out.start()
    moves[1].wait()
    store_gain(joined, own_gain[...])
    for move in moves[2:]:
        move.wait()
    out.wait()


def held_in_hbm(*arrays):
    return [pltpu.with_memory_space_constraint(array, pltpu.HBM) for array in arrays]


def opening(hidden, gain, weights, peers):
    many = (peers, hidden.shape[0] // 2, LANES)
    joined = (sum(array.size for array in weights) // LANES + GAIN_ROWS, LANES)
    pieces = sum(array.shape[1] for array in weights) // LANES
    operands = held_in_hbm(hidden, gain[None], *weights)
    return pl.pallas_call(
        open_kernel,
        out_shape=(
            jax.ShapeDtypeStruct(many, jnp.bfloat16),
            pltpu.VMEM(joined, jnp.bfloat16),
        ),
        in_specs=[IN_HBM] * len(operands),
        out_specs=(IN_HBM, IN_VMEM),
        scratch_shapes=[
            pltpu.VMEM(hidden.shape, jnp.bfloat16),
            pltpu.VMEM((1, LANES), jnp.float32),
            pltpu.VMEM(many, jnp.bfloat16),
            pltpu.SemaphoreType.DMA((pieces + 3,)),
        ],
        compiler_params=pltpu.CompilerParams(vmem_limit_bytes=8 << 20),
        cost_estimate=pl.CostEstimate(flops=2_000_000, bytes_accessed=1_000_000, transcendentals=0),
        name="opening",
    )(*operands)


def later_kernel(decay, inverse, lengths, gain, *refs):
    *sources, joined, table, place, own_gain, arrived = refs
    pairs, at = [(lengths, place), (gain, own_gain)], 0
    for source in sources:
        pairs.append((source, joined.at[at : at + source.shape[0]]))
        at += source.shape[0]
    moves = started(pairs, arrived)
    lane = lax.broadcasted_iota(jnp.int32, (1, LANES), 1)
    moves[0].wait()
    moves[1].wait()
    store_gain(joined, own_gain[...])
    seqs = place.shape[0]
    for i in range(seqs):
        angle = place[i].astype(jnp.float32) * inverse[...]
        filled = lax.rem(place[i], BLOCK)
        distance = (filled - lane).astype(jnp.float32)
        table[i : i + 1] = jnp.cos(angle)
        table[seqs + i : seqs + i + 1] = jnp.sin(angle)
        table[2 * seqs + i : 2 * seqs + i + 1] = jnp.where(
            lane < filled, jnp.exp(-decay[0] * distance), 0.0
        )
        reach = (filled + 1 + 0 * lane).astype(jnp.float32)
        table[3 * seqs + i : 3 * seqs + i + 1] = jnp.exp(-decay[0] * reach)
    for move in moves[2:]:
        move.wait()


def join_later(decay, lengths, gain, weights):
    inverse = 10000.0 ** (-jnp.arange(LANES, dtype=jnp.float32) / LANES)
    operands = held_in_hbm(lengths, gain[None], *weights)
    depth = sum(array.shape[0] for array in weights) + GAIN_ROWS
    return pl.pallas_call(
        later_kernel,
        out_shape=(
            pltpu.VMEM((depth, LANES), jnp.bfloat16),
            pltpu.VMEM((4 * lengths.shape[0], LANES), jnp.float32),
        ),
        in_specs=[IN_SMEM, IN_VMEM] + [IN_HBM] * len(operands),
        out_specs=(IN_VMEM, IN_VMEM),
        scratch_shapes=[
            pltpu.SMEM(lengths.shape, jnp.int32),
            pltpu.VMEM((1, LANES), jnp.float32),
            pltpu.SemaphoreType.DMA((len(operands),)),
        ],
        compiler_params=pltpu.CompilerParams(vmem_limit_bytes=8 << 20),
        cost_estimate=pl.CostEstimate(flops=2_000_000, bytes_accessed=1_000_000, transcendentals=0),
        name="later",
    )(decay, inverse[None], *operands)


def rotated_by(vectors, cosine, sine):
    half = cosine.shape[1]
    front, back = vectors[:, :half], vectors[:, half:]
    return jnp.concatenate([front * cosine - back * sine, front * sine + back * cosine], axis=1)


def of_each(row, products):
    result = products[0]
    for i, product in enumerate(products[1:], 1):
        result = jnp.where(row == i, product, result)
    return result


def retain_kernel(arrived, table, state, keys, values, group_gain, mixed):
    seqs, _, key_width, value_width = state.shape
    total = arrived[0].astype(jnp.float32)
    for i in range(1, arrived.shape[0]):
        total = total + arrived[i].astype(jnp.float32)
    ends = 2 * (key_width + value_width)
    scale = lax.rsqrt(total[:, ends : ends + 1] / D + epsilon)
    ready = (scale * total[:, :ends]).astype(jnp.bfloat16).astype(jnp.float32)
    cosine, sine = table[:seqs], table[seqs : 2 * seqs]
    weighting = table[2 * seqs : 3 * seqs]
    carried = table[3 * seqs :, :1]
    query = rotated_by(ready[:, :key_width], cosine, sine).astype(jnp.bfloat16)
    fresh = rotated_by(ready[:, key_width : 2 * key_width], cosine, sine) * key_width ** (-0.5)
    value = ready[:, 2 * key_width : 2 * key_width + value_width]
    gate = ready[:, 2 * key_width + value_width :]
    own = jnp.sum(query.astype(jnp.float32) * fresh, axis=1, keepdims=True) * value
    row_k = lax.broadcasted_iota(jnp.int32, (seqs, keys.shape[2]), 0)
    row_v = lax.broadcasted_iota(jnp.int32, (seqs, value_width), 0)
    scores = of_each(row_k, [transposed_dot(query, keys[i, 0]) for i in range(seqs)])
    block_weights = (scores * weighting).astype(jnp.bfloat16)
    block = of_each(row_v, [wide_dot(block_weights, values[i, 0]) for i in range(seqs)])
    remembered = []
    for i in range(seqs):
        high = state[i, 0].astype(jnp.bfloat16)
        low = (state[i, 0] - high.astype(jnp.float32)).astype(jnp.bfloat16)
        remembered.append(wide_dot(query, high) + wide_dot(query, low))
    retained = own + block + carried * of_each(row_v, remembered)
    centre = jnp.mean(retained, axis=1, keepdims=True)
    away = retained - centre
    spread = jnp.mean(away * away, axis=1, keepdims=True)
    normed = away * lax.rsqrt(spread + epsilon)
    result = (jax.nn.silu(gate) * normed * group_gain[...]).astype(jnp.bfloat16)
    for i in range(mixed.shape[0]):
        mixed[i] = result


def retain(arrived, table, state, keys, values, group_gain):
    seqs, _, _, value_width = state.shape
    out_shape = jax.ShapeDtypeStruct((arrived.shape[0], seqs, value_width), jnp.bfloat16)
    operands = (arrived, table, state, keys, values, group_gain[None])
    return call(retain_kernel, out_shape, operands, [])


def activate_kernel(units, pad, arrived, activated):
    total = arrived[0].astype(jnp.float32)
    for i in range(1, arrived.shape[0]):
        total = total + arrived[i].astype(jnp.float32)
    scale = lax.rsqrt(total[:, units : units + 1] / D + epsilon)
    gate, up = scale * total[:, :units], scale * total[:, units + pad :]
    result = (jax.nn.silu(gate) * up).astype(jnp.bfloat16)
    for i in range(activated.shape[0]):
        activated[i] = result


def activate(arrived, units, pad):
    out_shape = jax.ShapeDtypeStruct((*arrived.shape[:2], units), jnp.bfloat16)
    kernel = functools.partial(activate_kernel, units, pad)
    return call(kernel, out_shape, (arrived,), [])


def transposed_dot(left, right):
    return lax.dot_general(
        left, right, (((1,), (1,)), ((), ())), preferred_element_type=jnp.float32
    )


def store_by_peer(terms, wide, first):
    peers, half, _ = terms.shape
    for i in range(peers):
        at = half * ((i + first) % peers)
        terms[i] = wide[at : at + half].astype(jnp.bfloat16)


def gathered_rows(arrived, wide, first):
    peers, half, _ = arrived.shape
    for i in range(peers):
        at = half * ((i + first) % peers)
        wide[at : at + half] = arrived[i].astype(jnp.float32)


def project_kernel(arrived, own, partner, terms, stream, wide):
    _, rows, features = stream.shape
    half = terms.shape[1]
    width = wide.shape[1] - LANES
    side = lax.axis_index("core")
    place = side if SPREAD_SIDES[0] == 0 else 1 - side
    for i in range(rows // half):
        span = slice(half * i, half * (i + 1))
        source = (i - SPREAD_AT) % (rows // half)
        stream[0, span] = arrived[place, source].astype(jnp.float32)
        stream[1, span] = arrived[1 - place, source].astype(jnp.float32)
    parts = [stream[i] for i in range(2)]
    scaled = jnp.concatenate(
        [
            (part * from_thirds(weights[weights.shape[0] - GAIN_ROWS :])).astype(jnp.bfloat16)
            for part, weights in zip(parts, (own, partner))
        ],
        axis=1,
    )
    for i in range(width // LANES):
        span = slice(features * i, features * (i + 1))
        columns = jnp.concatenate([own[span], partner[span]], axis=0)
        wide[:, LANES * i : LANES * (i + 1)] = wide_dot(scaled, columns)
    squares = jnp.sum(parts[0] * parts[0] + parts[1] * parts[1], axis=1, keepdims=True)
    lane = lax.broadcasted_iota(jnp.int32, (rows, LANES), 1)
    wide[:, width:] = jnp.where(lane == 0, squares, 0.0)
    store_by_peer(terms, wide, HEADS_AT)


def call(kernel, out_shape, operands, scratch):
    return pl.pallas_call(
        kernel,
        out_shape=out_shape,
        in_specs=[IN_VMEM] * len(operands),
        out_specs=jax.tree.map(lambda _: IN_VMEM, out_shape),
        scratch_shapes=scratch,
        compiler_params=pltpu.CompilerParams(vmem_limit_bytes=8 << 20),
        cost_estimate=pl.CostEstimate(flops=8_000_000, bytes_accessed=1_000_000, transcendentals=0),
    )(*operands)


def project(arrived, own, partner, z):
    _, kv, half, features = arrived.shape
    rows = kv * half
    width = (own.shape[0] - GAIN_ROWS) * LANES // features + LANES
    out_shape = (
        jax.ShapeDtypeStruct((z, rows // z, width), jnp.bfloat16),
        jax.ShapeDtypeStruct((2, rows, features), jnp.float32),
    )
    scratch = [pltpu.VMEM((rows, width), jnp.float32)]
    return call(project_kernel, out_shape, (arrived, own, partner), scratch)


def mix_kernel(head, arrived, own, partner, terms, wide):
    gathered_rows(arrived, wide, MIXED_AT)
    every = wide[...].astype(jnp.bfloat16)
    span = slice(head, head + wide.shape[1])
    both = jnp.concatenate([wide_dot(every, own[span]), wide_dot(every, partner[span])], axis=1)
    both = both.astype(jnp.bfloat16)
    for i in range(terms.shape[0]):
        terms[i] = both


def mix(arrived, own, partner, head, kv):
    z, half, width = arrived.shape
    rows = z * half
    out_shape = jax.ShapeDtypeStruct((kv, rows, 2 * LANES), jnp.bfloat16)
    scratch = [pltpu.VMEM((rows, width), jnp.float32)]
    return call(functools.partial(mix_kernel, head), out_shape, (arrived, own, partner), scratch)


def finish_kernel(down, arrived, own, partner, residual, sent, wide):
    gathered_rows(arrived, wide, ACTIVE_AT)
    every = wide[...].astype(jnp.bfloat16)
    span = slice(down, down + wide.shape[1])
    side = lax.axis_index("core")
    place = side if RETURN_SIDES[0] == 0 else 1 - side
    peers, half, _ = sent.shape
    for i, weights in enumerate((own, partner)):
        total = wide_dot(every, weights[span]) + residual[i]
        to = place if i == 0 else 1 - place
        for peer in range(peers // 2):
            at = half * ((peer + RETURN_AT) % (peers // 2))
            sent[to * (peers // 2) + peer] = total[at : at + half]


def finish(arrived, own, partner, residual, down, kv):
    z, half, width = arrived.shape
    rows = z * half
    out_shape = jax.ShapeDtypeStruct((2 * kv, rows // kv, LANES), jnp.float32)
    scratch = [pltpu.VMEM((rows, width), jnp.float32)]
    return call(
        functools.partial(finish_kernel, down),
        out_shape,
        (arrived, own, partner, residual),
        scratch,
    )


def channel_kernel(
    head, units, pad, parts, stream, own_weights, partner, terms, residual, wide
):
    rows, features = stream.shape[1:]
    half = terms.shape[1]
    mixer_out = parts[0].astype(jnp.float32)
    for i in range(1, parts.shape[0]):
        mixer_out = mixer_out + parts[i].astype(jnp.float32)
    own = stream[0] + mixer_out[:, :features]
    other = stream[1] + mixer_out[:, features:]
    end = partner.shape[0]
    scaled_own, scaled_other = (
        (part * from_thirds(weights[end - GAIN_ROWS :])).astype(jnp.bfloat16)
        for part, weights in ((own, own_weights), (other, partner))
    )
    squares = jnp.sum(own * own + other * other, axis=1, keepdims=True)
    wide[:, :units] = transposed_dot(
        scaled_own, own_weights[head : head + units]
    ) + transposed_dot(
        scaled_other, partner[head : head + units]
    )
    lane = lax.broadcasted_iota(jnp.int32, (rows, pad), 1)
    wide[:, units : units + pad] = jnp.where(lane == 0, squares, 0.0)
    wide[:, units + pad :] = transposed_dot(
        scaled_own, own_weights[head + units : head + 2 * units]
    ) + transposed_dot(
        scaled_other, partner[head + units : head + 2 * units]
    )
    store_by_peer(terms, wide, UNITS_AT)
    row = lax.broadcasted_iota(jnp.int32, (rows, features), 0)
    here = row // half == lax.axis_index("kv")
    residual[0] = jnp.where(here, own, 0.0)
    residual[1] = jnp.where(here, other, 0.0)


def channel(parts, stream, own_weights, partner, head, units, z):
    pad = -units % LANES
    _, rows, features = stream.shape
    width = 2 * units + pad
    out_shape = (
        jax.ShapeDtypeStruct((z, rows // z, width), jnp.bfloat16),
        jax.ShapeDtypeStruct((2, rows, features), jnp.float32),
    )
    return call(
        functools.partial(channel_kernel, head, units, pad),
        out_shape,
        (parts, stream, own_weights, partner),
        [pltpu.VMEM((rows, width), jnp.float32)],
    )


def local(
    hidden_in,
    mixer_gain,
    query_weight,
    key_weight,
    value_weight,
    gate_weight,
    decay_rate,
    prior_state,
    key_block,
    value_block,
    lengths,
    group_gain,
    output_weight,
    channel_gain,
    hidden_gate,
    hidden_up,
    hidden_down,
):
    kv, z = lax.axis_size("kv"), lax.axis_size("z")
    own_rows, features = hidden_in.shape
    half = own_rows // 2
    head_width, units = output_weight.shape[0], hidden_gate.shape[1]
    spread, back = (
        [side * kv + member for side in sides for member in turned(kv, first)]
        for sides, first in ((SPREAD_SIDES, SPREAD_AT), (RETURN_SIDES, RETURN_AT))
    )
    sent, first = opening(
        hidden_in, mixer_gain, (query_weight, key_weight, value_weight, gate_weight), 2 * kv
    )
    rows = exchange(sent, ("core", "kv"), spread).reshape(2, kv, half, features)
    first_partner = from_partner(first)
    terms, stream = project(rows, first, first_partner, z)
    arrived = exchange(terms, "z", turned(z, HEADS_AT))
    later = (output_weight, hidden_gate.T, hidden_up.T, hidden_down)
    own, table = join_later(decay_rate, lengths, channel_gain, later)
    partner = from_partner(own)
    mixed = retain(arrived, table, prior_state, key_block, value_block, group_gain)
    mixed = exchange(mixed, "z", turned(z, MIXED_AT))
    parts = exchange(mix(mixed, own, partner, 0, kv), "kv", turned(kv, SUM_AT))
    terms, residual = channel(parts, stream, own, partner, head_width, units, z)
    activated = activate(exchange(terms, "z", turned(z, UNITS_AT)), units, -units % LANES)
    total = finish(
        exchange(activated, "z", turned(z, ACTIVE_AT)), own, partner, residual, head_width + 2 * units, kv
    )
    total = exchange(total, ("core", "kv"), back).reshape(2, kv, half, features)
    total = total if RETURN_SIDES[0] == 0 else total[::-1]
    return jnp.sum(total, axis=1).reshape(own_rows, features).astype(jnp.bfloat16)


def solution(mesh):
    kv, tp = mesh.shape["kv"], mesh.shape["tp"]
    chips = Mesh(mesh.devices.reshape(kv, tp // 2, 2), ("kv", "z", "core"))
    tp = ("z", "core")
    in_specs = (
        P("kv", tp),
        P(tp),
        P(tp, "kv"),
        P(tp, "kv"),
        P(tp, "kv"),
        P(tp, "kv"),
        P("kv"),
        P(tp, "kv", None, None),
        P(tp, "kv", None, None),
        P(tp, "kv", None, None),
        P(tp),
        P("kv"),
        P("kv", tp),
        P(tp),
        P(tp, "kv"),
        P(tp, "kv"),
        P("kv", tp),
    )
    return jax.shard_map(
        local, mesh=chips, in_specs=in_specs, out_specs=P("kv", tp), check_vma=False
    )
```
